256 devices in a mesh: ep: 32 (over z, x), tp: 8 (over y, core).
Axes of the slice: x: 4, y: 4, z: 8, core: 2. Of those that a mesh axis runs over, the one named last changes fastest.
Arguments:
- tokens: bfloat16 [3072, 4096], P('ep'), may hold values from -6 to 6
- mix_gain: float32 [4096], replicated, may hold values from 0.1 to 1.9
- ffn_gain: float32 [4096], replicated, may hold values from 0.1 to 1.9
- in_proj: bfloat16 [4096, 1024], P(None, 'tp'), may hold values from -0.09375 to 0.09375
- decay_rate: float32 [64, 64], P('tp'), may hold values from 0.05 to 2
- frequency: float32 [64, 64], P('tp'), may hold values from -3 to 3
- log_step: float32 [64], P('tp'), may hold values from -3 to 0.5
- b_real: float32 [64, 64, 16], P('tp'), may hold values from -1.5 to 1.5
- b_imag: float32 [64, 64, 16], P('tp'), may hold values from -1.5 to 1.5
- c_real: float32 [64, 16, 64], P('tp'), may hold values from -0.75 to 0.75
- c_imag: float32 [64, 16, 64], P('tp'), may hold values from -0.75 to 0.75
- skip_gain: float32 [1024], P('tp'), may hold values from -5 to 5
- states: float32 [2, 3072, 4096], P(None, 'ep', 'tp'), may hold values from -6 to 6
- out_proj: bfloat16 [1024, 4096], P('tp'), may hold values from -0.1875 to 0.1875
- route_ids: int32 [3072, 2], P('ep'), may hold values from 0 to 31, all different within a row; in each aligned block of 96 rows (0 to 95, 96 to 191, ...) at most 12 rows name the same one
- route_logits: float32 [3072, 2], P('ep'), may hold values from -5 to 5
- expert_gate: bfloat16 [32, 4096, 3072], P('ep', None, 'tp'), may hold values from -0.09375 to 0.09375
- expert_up: bfloat16 [32, 4096, 3072], P('ep', None, 'tp'), may hold values from -0.09375 to 0.09375
- expert_down: bfloat16 [32, 3072, 4096], P('ep', 'tp'), may hold values from -0.109375 to 0.109375
- dense_gate: bfloat16 [4096, 6144], P('tp', 'ep'), may hold values from -0.09375 to 0.09375
- dense_up: bfloat16 [4096, 6144], P('tp', 'ep'), may hold values from -0.09375 to 0.09375
- dense_down: bfloat16 [6144, 4096], P('ep', 'tp'), may hold values from -0.078125 to 0.078125
- branch_gate: bfloat16 [4096], replicated, may hold values from -0.09375 to 0.09375
Outputs:
- output: bfloat16 [3072, 4096], P('ep', 'tp')
- new_states: float32 [2, 3072, 4096], P(None, 'ep', 'tp')
The draws below stay inside these ranges and needn't reach their ends.
Inputs may be any that keep to these rules, and one draw needn't show every extreme that they name: `route_ids`: each row names 2 different experts; among the rows of one device (aligned blocks of 96 rows) no expert is named by more than 12 rows.
All inputs are finite; a program needn't handle non-finite values.
Results may differ from the reference program's by a relative error of at most 0.017.
Values may be sent and summed in bfloat16 or wider, within the bound.
A program may use at most 128 MiB of HBM per device.

```python
import math
import jax
import jax.numpy as jnp
import numpy as np
from jax import lax

D = 4096
S5W = 1024
GROUP = 16
GROUPS = 64
STATE = 64
FFE = 3072
FFD = 6144
TOPK = 2
SEQ_DEV = 96
BATCH = 3072
EXPERTS = 32
CAP = 12
N_EP = 32
N_TP = 8


def steps_of(own_key, dims, cuts, least, top_value):
    loudness, own = 1.0, jax.random.fold_in(own_key, 6)
    for axis_at, blocks in cuts:
        steps = jnp.exp(jax.random.uniform(jax.random.fold_in(own, axis_at), (blocks,), jnp.float32, least / len(cuts), top_value / len(cuts)))
        loudness = loudness * jnp.repeat(steps, dims[axis_at] // blocks).reshape([-1 if axis == axis_at else 1 for axis in range(len(dims))])
    return loudness


def deal_out(key, own, number, rows, number_of, top, bound, slope):
    sequence = jax.random.permutation(key, number_of)
    crowded, ordinary = portions_of(number_of, rows * top, bound, slope, True), portions_of(number_of, rows * top, bound, slope, False)
    places = jnp.arange(number_of)

    def named(lengths, turn):
        used = int((lengths > 0).sum())
        fixed = max(1, used // 4)
        passed = fixed + (places - fixed + turn * (used - fixed)) % max(1, number_of - fixed)
        return jnp.zeros((number_of,), jnp.int32).at[sequence[jnp.where(places < fixed, places, passed)]].set(jnp.asarray(lengths, jnp.int32))

    lengths = jnp.where(number % 4 == 0, named(crowded, number // 4), named(ordinary, number - number // 4 - 1))
    mixed = jax.random.permutation(jax.random.fold_in(own, 3), number_of)
    donor, receiver = mixed[0:number_of // 2 * 2:2], mixed[1:number_of // 2 * 2:2]
    slack = jnp.minimum(lengths[donor] - 1, bound - lengths[receiver]) // 2
    slack = jnp.where((donor == sequence[0]) | (receiver == sequence[0]) | (lengths[receiver] == 0), 0, jnp.maximum(slack, 0))
    passed = jax.random.randint(jax.random.fold_in(own, 4), (number_of // 2,), 0, 1 << 20) % (slack + 1)
    lengths = lengths.at[donor].add(-passed).at[receiver].add(passed)
    labels = jnp.searchsorted(jnp.cumsum(lengths), jnp.arange(rows * top), side="right").astype(jnp.int32)
    listing = labels.reshape(top, rows).T
    listing = listing[jax.random.permutation(jax.random.fold_in(own, 1), rows)]
    turn = jax.random.randint(jax.random.fold_in(own, 2), (rows, 1), 0, top)
    return jnp.take_along_axis(listing, (jnp.arange(top)[None, :] + turn) % top, axis=1)


def portions_of(amount, total, bound, slope, full):
    weights = [(1 << 20) // math.isqrt(standing ** slope) + 1 for standing in range(1, amount + 1)]
    largest = bound if full else min(bound, max(-(-total // amount), total * weights[0] // sum(weights)))
    least = 1 if total - largest >= amount - 1 else 0
    counts, rest = [largest] + [least] * (amount - 1), total - largest - least * (amount - 1)
    while rest > 0:
        free = [i for i in range(1, amount) if counts[i] < largest] or [i for i in range(1, amount) if counts[i] < bound]
        mass, budget = sum([weights[i] for i in free]), rest
        for i in free:
            addition = min(bound - counts[i], max(1, budget * weights[i] // mass), rest)
            counts[i] = counts[i] + addition
            rest = rest - addition
    return np.array(counts)


def noise(rng, extent, width, bound, pieces=(), kind=jnp.bfloat16):
    loudness = steps_of(rng, extent, pieces, -0.22, 0.18) if pieces else 1.0
    values = jax.random.normal(rng, extent, jnp.float32) * width * loudness
    return jnp.minimum(jnp.maximum(values, -bound), bound).astype(kind)


def setup_inputs(seed: int = 0) -> dict:
    seeds = jax.random.split(jax.random.key(seed), 24)
    tokens = noise(seeds[0], (BATCH, D), 1.0, 6.0, ((0, 32),))
    mix_gain = jnp.clip(1.0 + 0.18 * jax.random.normal(seeds[1], (D,), jnp.float32), 0.1, 1.9)
    ffn_gain = jnp.clip(1.0 + 0.18 * jax.random.normal(seeds[2], (D,), jnp.float32), 0.1, 1.9)
    in_proj = noise(seeds[3], (D, S5W), D ** -0.5, 0.09375, ((1, 8),))
    decay_rate = jnp.clip(jnp.exp(math.log(2.0) - 3.6888794 * jax.random.uniform(seeds[4], (GROUPS, STATE), jnp.float32) ** steps_of(seeds[4], (GROUPS, STATE), ((0, 8),), -0.2, 0.2)), 0.05, 2.0)
    frequency = jnp.clip(jax.random.uniform(seeds[5], (GROUPS, STATE), jnp.float32, -3.0, 3.0) * steps_of(seeds[5], (GROUPS, STATE), ((0, 8),), -0.4, 0.0), -3.0, 3.0)
    log_step = jnp.clip(-3.0 + 3.5 * jax.random.uniform(seeds[6], (GROUPS,), jnp.float32) ** steps_of(seeds[6], (GROUPS,), ((0, 8),), -0.2, 0.2), -3.0, 0.5)
    b_real = noise(seeds[7], (GROUPS, STATE, GROUP), GROUP ** -0.5, 1.5, ((0, 8),), jnp.float32)
    b_imag = noise(seeds[8], (GROUPS, STATE, GROUP), GROUP ** -0.5, 1.5, ((0, 8),), jnp.float32)
    c_real = noise(seeds[9], (GROUPS, GROUP, STATE), STATE ** -0.5, 0.75, ((0, 8),), jnp.float32)
    c_imag = noise(seeds[10], (GROUPS, GROUP, STATE), STATE ** -0.5, 0.75, ((0, 8),), jnp.float32)
    skip_gain = noise(seeds[11], (S5W,), 1.0, 5.0, ((0, 8),), jnp.float32)
    states = noise(seeds[12], (2, BATCH, GROUPS * STATE), 1.0, 6.0, ((1, 32), (2, 8)), jnp.float32)
    out_proj = noise(seeds[13], (S5W, D), S5W ** -0.5, 0.1875, ((0, 8),))
    route_ids_keys = jax.random.split(jax.random.fold_in(seeds[14], 1), BATCH // SEQ_DEV)
    route_ids_turns = jax.random.permutation(jax.random.fold_in(seeds[14], 3), BATCH // SEQ_DEV)
    route_ids = jax.vmap(lambda own, number: deal_out(jax.random.fold_in(seeds[14], 2), own, number, SEQ_DEV, EXPERTS, TOPK, CAP, 2))(route_ids_keys, route_ids_turns).reshape((BATCH, TOPK))
    route_logits = noise(seeds[15], (BATCH, TOPK), 1.0, 5.0, ((0, 32),), jnp.float32)
    expert_gate = noise(seeds[16], (EXPERTS, D, FFE), D ** -0.5, 0.09375, ((0, 32), (2, 8)))
    expert_up = noise(seeds[17], (EXPERTS, D, FFE), D ** -0.5, 0.09375, ((0, 32), (2, 8)))
    expert_down = noise(seeds[18], (EXPERTS, FFE, D), FFE ** -0.5, 0.109375, ((0, 32), (1, 8)))
    dense_gate = noise(seeds[19], (D, FFD), D ** -0.5, 0.09375, ((0, 8), (1, 32)))
    dense_up = noise(seeds[20], (D, FFD), D ** -0.5, 0.09375, ((0, 8), (1, 32)))
    dense_down = noise(seeds[21], (FFD, D), FFD ** -0.5, 0.078125, ((0, 32), (1, 8)))
    branch_gate = noise(seeds[22], (D,), D ** -0.5, 0.09375)
    return dict(tokens=tokens, mix_gain=mix_gain, ffn_gain=ffn_gain, in_proj=in_proj, decay_rate=decay_rate, frequency=frequency, log_step=log_step, b_real=b_real, b_imag=b_imag, c_real=c_real, c_imag=c_imag, skip_gain=skip_gain, states=states, out_proj=out_proj, route_ids=route_ids, route_logits=route_logits, expert_gate=expert_gate, expert_up=expert_up, expert_down=expert_down, dense_gate=dense_gate, dense_up=dense_up, dense_down=dense_down, branch_gate=branch_gate)


def rms_norm(values, gain):
    flt = values.astype(jnp.float32)
    scaled = flt * lax.rsqrt(lax.optimization_barrier(jnp.mean(flt * flt, axis=-1, keepdims=True)) + 1e-06)
    return (scaled * gain.astype(jnp.float32)).astype(jnp.bfloat16)

def discretize(decay_rate, frequency, log_step, b_real, b_imag):
    step_size = jnp.exp(log_step)[:, None]
    lam_re = -decay_rate
    lam_im = frequency
    magnitude = jnp.exp(lam_re * step_size)
    abar_re = magnitude * jnp.cos(lam_im * step_size)
    abar_im = magnitude * jnp.sin(lam_im * step_size)
    denom = lam_re * lam_re + lam_im * lam_im
    fac_re = ((abar_re - 1.0) * lam_re + abar_im * lam_im) / denom
    fac_im = (abar_im * lam_re - (abar_re - 1.0) * lam_im) / denom
    bbar_re = fac_re[..., None] * b_real - fac_im[..., None] * b_imag
    bbar_im = fac_re[..., None] * b_imag + fac_im[..., None] * b_real
    return (abar_re, abar_im, bbar_re, bbar_im)

def state_step(drive, states, decay_rate, frequency, log_step, b_real, b_imag, c_real, c_imag, skip_gain):
    count = drive.shape[0]
    groups = decay_rate.shape[0]
    abar_re, abar_im, bbar_re, bbar_im = discretize(decay_rate, frequency, log_step, b_real, b_imag)
    grouped = drive.astype(jnp.float32).reshape(count, groups, GROUP)
    old_re = states[0].reshape(count, groups, STATE)
    old_im = states[1].reshape(count, groups, STATE)
    high = lax.Precision.HIGHEST
    push_re = jnp.einsum('ngh,gph->ngp', grouped, bbar_re, precision=high)
    push_im = jnp.einsum('ngh,gph->ngp', grouped, bbar_im, precision=high)
    new_re = abar_re * old_re - abar_im * old_im + push_re
    new_im = abar_re * old_im + abar_im * old_re + push_im
    readout = jnp.einsum('ngp,ghp->ngh', new_re, c_real, precision=high) - jnp.einsum('ngp,ghp->ngh', new_im, c_imag, precision=high) + skip_gain.reshape(groups, GROUP) * grouped
    reads = jax.nn.gelu(readout.reshape(count, groups * GROUP)).astype(jnp.bfloat16)
    fresh = jnp.stack([new_re.reshape(count, groups * STATE), new_im.reshape(count, groups * STATE)])
    return (reads, fresh)

def reference(tokens, mix_gain, ffn_gain, in_proj, decay_rate, frequency, log_step, b_real, b_imag, c_real, c_imag, skip_gain, states, out_proj, route_ids, route_logits, expert_gate, expert_up, expert_down, dense_gate, dense_up, dense_down, branch_gate):
    normed = rms_norm(tokens, mix_gain)
    drive = jnp.dot(normed, in_proj, preferred_element_type=jnp.float32).astype(jnp.bfloat16)
    reads, new_states = state_step(drive, states, decay_rate, frequency, log_step, b_real, b_imag, c_real, c_imag, skip_gain)
    block_width = S5W // N_TP
    mixed = jnp.zeros((BATCH, D), jnp.float32)
    for block in range(N_TP):
        piece = jnp.dot(reads[:, block * block_width:(block + 1) * block_width], out_proj[block * block_width:(block + 1) * block_width], preferred_element_type=jnp.float32).astype(jnp.bfloat16)
        mixed = mixed + piece.astype(jnp.float32)
    mixed = mixed.astype(jnp.bfloat16)
    resid = (tokens.astype(jnp.float32) + mixed.astype(jnp.float32)).astype(jnp.bfloat16)
    normed_two = rms_norm(resid, ffn_gain)
    route_weights = jax.nn.softmax(route_logits, axis=-1)
    blocked_ids = route_ids.reshape(N_EP, SEQ_DEV * TOPK)
    onehot = (blocked_ids[..., None] == jnp.arange(EXPERTS, dtype=jnp.int32)[None, None, :]).astype(jnp.int32)
    rank = jnp.cumsum(onehot, axis=1) - onehot
    slot = lax.optimization_barrier(jnp.sum(rank * onehot, axis=-1))
    block_index = jnp.arange(N_EP, dtype=jnp.int32)[:, None]
    position = blocked_ids * (N_EP * CAP) + block_index * CAP + slot
    token_index = block_index * SEQ_DEV + jnp.arange(SEQ_DEV * TOPK, dtype=jnp.int32)[None, :] // TOPK
    table = jnp.full((EXPERTS * N_EP * CAP,), BATCH, jnp.int32).at[position.reshape(-1)].set(token_index.reshape(-1))
    padded = jnp.concatenate([normed_two, jnp.zeros((1, D), jnp.bfloat16)], axis=0)
    hidden_block = FFE // N_TP

    def one_expert(inputs):
        index_row, gate_w, up_w, down_w = inputs
        rows_in = padded[index_row]
        summed = jnp.zeros((N_EP * CAP, D), jnp.float32)
        for block in range(N_TP):
            lo = block * hidden_block
            gate_val = jnp.dot(rows_in, gate_w[:, lo:lo + hidden_block], preferred_element_type=jnp.float32)
            up_val = jnp.dot(rows_in, up_w[:, lo:lo + hidden_block], preferred_element_type=jnp.float32)
            hidden = (jax.nn.silu(gate_val) * up_val).astype(jnp.bfloat16)
            piece = jnp.dot(hidden, down_w[lo:lo + hidden_block], preferred_element_type=jnp.float32)
            summed = summed + piece.astype(jnp.bfloat16).astype(jnp.float32)
        return summed.astype(jnp.bfloat16)
    expert_out = lax.map(one_expert, (table.reshape(EXPERTS, N_EP * CAP), expert_gate, expert_up, expert_down))
    picked = expert_out.reshape(EXPERTS * N_EP * CAP, D)[position.reshape(-1)]
    picked = picked.reshape(BATCH, TOPK, D).astype(jnp.float32)
    routed = lax.optimization_barrier(jnp.sum(route_weights[..., None] * picked, axis=1))
    gate_val = jnp.dot(normed_two, dense_gate, preferred_element_type=jnp.float32)
    up_val = jnp.dot(normed_two, dense_up, preferred_element_type=jnp.float32)
    dense_hidden = (jax.nn.silu(gate_val) * up_val).astype(jnp.bfloat16)
    dense_term = jnp.dot(dense_hidden, dense_down, preferred_element_type=jnp.float32)
    branch = jax.nn.sigmoid(jnp.dot(normed_two, branch_gate, preferred_element_type=jnp.float32))
    output = (resid.astype(jnp.float32) + routed + branch[:, None] * dense_term).astype(jnp.bfloat16)
    return (output, new_states)
```

```python
import functools
import heapq

import jax
import jax.numpy as jnp
from jax import lax
from jax.experimental import pallas as pl
from jax.experimental.pallas import tpu as pltpu
from jax.sharding import Mesh
from jax.sharding import PartitionSpec as P

GROUP = 16
STATE = 64
EP = ("ep_0", "ep_1")
MESH = pl.DeviceIdType.MESH


class Node:
    def __init__(self, chunk, off, parent, move):
        self.chunk, self.off, self.parent, self.move = chunk, off, parent, move
        self.kids = []
        if parent is not None:
            parent.kids.append(self)


def ring_offsets(size, far_up):
    up = size // 2 if far_up else (size - 1) // 2
    return up, size - 1 - up


def chain(chunk, root, axis, name, size, far_up):
    up, down = ring_offsets(size, far_up)
    found = [root]
    for step, count in ((1, up), (-1, down)) if far_up else ((-1, down), (1, up)):
        last = root
        for _ in range(count):
            off = list(last.off)
            off[axis] += step
            last = Node(chunk, tuple(off), last, (name, step))
            found.append(last)
    return found


def ep_tree(sizes):
    nodes = []
    for chunk in range(2):
        first, second = (0, 1) if chunk == 0 else (1, 0)
        root = Node(chunk, (0, 0), None, None)
        line = chain(chunk, root, first, EP[first], sizes[first], True)
        for i, node in enumerate(line):
            nodes += chain(chunk, node, second, EP[second], sizes[second], i % 2 == 0)
    return nodes


def tp_tree(tp_count, chunks):
    nodes = []
    for chunk in range(chunks):
        root = Node(chunk, (0, 0), None, None)
        line = chain(chunk, root, 0, "y", tp_count // 2, chunk % 2 == 0)
        for node in line:
            nodes += [node, Node(chunk, (node.off[0], 1), node, ("core", 1))]
    return nodes


def timed(nodes, cost, lag):
    free, heap, order = {}, [], []
    for i, node in enumerate(nodes):
        if node.parent is None:
            node.sent, node.came = 0.0, 0.0
            heapq.heappush(heap, (0.0, i))
    place = {id(node): i for i, node in enumerate(nodes)}
    while heap:
        now, i = heapq.heappop(heap)
        node = nodes[i]
        order.append(node)
        for kid in node.kids:
            price = cost * (0.35 if kid.move[0] == "core" else 1.0)
            start = max(now, free.get(kid.move, 0.0))
            free[kid.move] = start + price
            kid.sent, kid.came = start, start + price + lag
            heapq.heappush(heap, (kid.came, place[id(kid)]))
    for i, node in enumerate(order):
        node.index = i
    return order


class Places:
    def __init__(self, kind, sizes):
        self.kind, self.sizes = kind, sizes
        if kind == "ep":
            self.me = (lax.axis_index("ep_0"), lax.axis_index("ep_1"))
        else:
            t = lax.axis_index("tp")
            self.me = (t // 2, t % 2)

    def shifted(self, off):
        return tuple(
            lax.rem(m + (o + s), s) for m, o, s in zip(self.me, off, self.sizes)
        )

    def flat(self, at):
        return at[0] * self.sizes[1] + at[1]

    def owner(self, off, sign=-1):
        return self.flat(self.shifted(tuple(sign * o for o in off)))

    def device(self, move, sign=1):
        name, step = move
        step = step * sign
        if self.kind == "ep":
            axis = EP.index(name)
            return {name: lax.rem(self.me[axis] + (step + self.sizes[axis]), self.sizes[axis])}
        off = (step, 0) if name == "y" else (0, step)
        return {"tp": self.flat(self.shifted(off))}

    def greet(self):
        barrier = pltpu.get_barrier_semaphore()
        moves = [("ep_0", 1), ("ep_0", -1), ("ep_1", 1), ("ep_1", -1)]
        if self.kind == "tp":
            moves = [("y", 1), ("y", -1), ("core", 1)]
        for move in moves:
            pl.semaphore_signal(barrier, inc=1, device_id=self.device(move), device_id_type=MESH)
        pl.semaphore_wait(barrier, len(moves))


def gather_events(order, places, source, target, send, recv, events, base=0.0):
    started = []

    def copy(node, src, device):
        own = places.owner(node.parent.off) if node.parent is not None else None
        return pltpu.make_async_remote_copy(
            src_ref=src,
            dst_ref=target(node.chunk, own),
            send_sem=send.at[node.index],
            recv_sem=recv.at[node.index],
            device_id=device,
            device_id_type=MESH,
        )

    def handle(node):
        if node.parent is None:
            src = source(node.chunk)
        else:
            src = target(node.chunk, places.owner(node.off))
            pltpu.make_async_remote_copy(
                src_ref=src,
                dst_ref=src,
                send_sem=send.at[node.index],
                recv_sem=recv.at[node.index],
                device_id=places.device(node.move),
                device_id_type=MESH,
            ).wait_recv()
        for kid in node.kids:
            moved = copy(kid, src, places.device(kid.move))
            moved.start()
            started.append(moved)

    for node in order:
        events.append((base + node.came, functools.partial(handle, node)))
    return started


def add_into(out, terms, rows, step=16):
    def body(i, _):
        at = pl.ds(pl.multiple_of(i * step, step), step)
        total = terms[0](at).astype(jnp.float32)
        for term in terms[1:]:
            total = total + term(at).astype(jnp.float32)
        out(at, total)
        return 0

    lax.fori_loop(0, rows // step, body, 0)


def reduce_events(order, places, view, load, put, slots, sums, rows, send, recv, events, base=0.0):
    started = []
    last = max(node.came for node in order)

    def handle(node):
        off = node.off
        own = places.owner(off)
        for kid in node.kids:
            slot = slots.at[kid.index]
            pltpu.make_async_remote_copy(
                src_ref=slot,
                dst_ref=slot,
                send_sem=send.at[kid.index],
                recv_sem=recv.at[kid.index],
                device_id=places.device(kid.move),
                device_id_type=MESH,
            ).wait_recv()
        terms = [lambda at: load(node.chunk, own, at)]
        for kid in node.kids:
            terms.append(lambda at, k=kid.index: slots[k, at, :])
        if node.parent is None:
            add_into(lambda at, v: put(node.chunk, at, v), terms, rows)
            return
        if node.kids:
            src = sums.at[node.index]

            def keep(at, v):
                sums[node.index, at, :] = v.astype(sums.dtype)

            add_into(keep, terms, rows)
        else:
            src = view(node.chunk, own)
        moved = pltpu.make_async_remote_copy(
            src_ref=src,
            dst_ref=slots.at[node.index],
            send_sem=send.at[node.index],
            recv_sem=recv.at[node.index],
            device_id=places.device(node.move, -1),
            device_id_type=MESH,
        )
        moved.start()
        started.append(moved)

    for node in reversed(order):
        events.append((base + last - node.came, functools.partial(handle, node)))
    return started


def run_events(events, started):
    for _, act in sorted(events, key=lambda pair: pair[0]):
        act()
    for group in started:
        for moved in group:
            moved.wait_send()


def vmem(count):
    return [pl.BlockSpec(memory_space=pltpu.VMEM)] * count


def dma_sems(order):
    return [pltpu.SemaphoreType.DMA((len(order),))] * 2


def params(collective_id):
    return pltpu.CompilerParams(collective_id=collective_id, has_side_effects=True)


def mix_kernel(
    tp_count, width, reads, weights, tokens, gain, gate, route,
    normed, resid, branch, held, stats, send, recv, send2, recv2,
):
    me = lax.axis_index("tp")
    barrier = pltpu.get_barrier_semaphore()
    others = [lax.rem(me + k, tp_count) for k in range(1, tp_count)]
    for other in others:
        pl.semaphore_signal(barrier, inc=1, device_id={"tp": other}, device_id_type=MESH)
    pl.semaphore_wait(barrier, tp_count - 1)

    def exchange(src, dst, send, recv):
        copies = []
        for k, other in enumerate(others):
            copies.append(
                pltpu.make_async_remote_copy(
                    src_ref=src,
                    dst_ref=dst.at[k + 1],
                    send_sem=send.at[k],
                    recv_sem=recv.at[k],
                    device_id={"tp": other},
                    device_id_type=MESH,
                )
            )
            copies[-1].start()
        return copies

    copies = exchange(reads, held, send, recv)
    depth = reads.shape[1]
    f32 = jnp.float32

    def part(value, k):
        owner = lax.rem(me + tp_count - k, tp_count)
        at = pl.ds(pl.multiple_of(owner * depth, depth), depth)
        return jnp.dot(value, weights[at, :], preferred_element_type=f32)

    total = part(reads[...], 0)
    for k, copy in enumerate(copies):
        copy.wait()
        total = total + part(held[k + 1], k + 1)
    flt = tokens[...].astype(f32) + total.astype(jnp.bfloat16).astype(f32)
    flt = flt.astype(jnp.bfloat16).astype(f32)
    resid[...] = flt.astype(jnp.bfloat16)
    gained = flt * gain[...]
    ones = jnp.ones((8, flt.shape[1]), f32)
    high = lax.Precision.HIGHEST
    turned = (((1,), (1,)), ((), ()))
    square = lax.dot_general(ones, flt * flt, turned, precision=high, preferred_element_type=f32)
    logit = lax.dot_general(
        ones, gained * gate[...], turned, precision=high, preferred_element_type=f32
    )
    rows = flt.shape[0]
    stats[0, 0, :, :rows] = square
    stats[0, 1, :, :rows] = logit
    copies = exchange(stats.at[0], stats, send2, recv2)
    for copy in copies:
        copy.wait()
    both = stats[0]
    for k in range(1, tp_count):
        both = both + stats[k]
    scale = lax.rsqrt(both[0, :, :rows] / width + 1e-06)
    branch[...] = route[...]
    branch[:1, :rows] = jax.nn.sigmoid(scale * both[1, :, :rows])[:1]
    first = (lax.broadcasted_iota(jnp.int32, (8, flt.shape[1]), 0) == 0).astype(f32)
    column = lax.dot_general(
        scale, first, (((0,), (0,)), ((), ())), precision=high, preferred_element_type=f32
    )
    value = (gained * column).astype(jnp.bfloat16)
    half = rows // 2
    normed[0] = value[:half]
    normed[1] = value[half:]


def mix(reads, weights, tokens, gain, gate, route, tp_count, width):
    rows, cols = tokens.shape
    bf16, f32 = jnp.bfloat16, jnp.float32
    return pl.pallas_call(
        functools.partial(mix_kernel, tp_count, width),
        out_shape=(
            jax.ShapeDtypeStruct((2, rows // 2, cols), bf16),
            jax.ShapeDtypeStruct((rows, cols), bf16),
            jax.ShapeDtypeStruct((8, 128), f32),
        ),
        in_specs=vmem(6),
        out_specs=tuple(vmem(3)),
        scratch_shapes=[
            pltpu.VMEM((tp_count, *reads.shape), bf16),
            pltpu.VMEM((tp_count, 2, 8, 128), f32),
        ]
        + [pltpu.SemaphoreType.DMA((tp_count - 1,))] * 4,
        compiler_params=params(1),
        name="mix",
    )(reads, weights, tokens, gain, gate, route)


def spread_kernel(order, small, sizes, block, extra, out, out_extra, send, recv, send2, recv2):
    places = Places("ep", sizes)
    places.greet()
    mine = places.flat(places.me)
    events = []
    one = gather_events(
        order, places, lambda c: block.at[c], lambda c, b: out.at[b, c], send, recv, events
    )
    two = gather_events(
        small, places, lambda c: extra, lambda c, b: out_extra.at[b], send2, recv2, events, 0.1
    )
    out[mine] = block[...]
    out_extra[mine] = extra[...]
    run_events(events, (one, two))


def spread(block, extra, sizes):
    count = sizes[0] * sizes[1]
    order = timed(ep_tree(sizes), 1.0, 1.8)
    small = timed([n for n in ep_tree(sizes) if n.chunk == 0], 0.1, 1.8)
    return pl.pallas_call(
        functools.partial(spread_kernel, order, small, sizes),
        out_shape=(
            jax.ShapeDtypeStruct((count, *block.shape), block.dtype),
            jax.ShapeDtypeStruct((count, *extra.shape), extra.dtype),
        ),
        in_specs=vmem(2),
        out_specs=tuple(vmem(2)),
        scratch_shapes=dma_sems(order) + dma_sems(small),
        compiler_params=params(2),
        name="spread",
    )(block, extra)


def expert_in_kernel(
    order, order2, order3, sizes, half, rows, wide,
    full, hid_all, mine, slots, sums, send, recv, send2, recv2, send3, recv3,
):
    places = Places("tp", sizes)
    places.greet()
    me = places.flat(places.me)
    part = rows.shape[2]
    span = rows.shape[1]
    events, f32 = [], jnp.float32

    def columns(b):
        return pl.ds(pl.multiple_of(b * part, part), part)

    def put(chunk, at, value):
        gate, up = value[:, :half], value[:, half:]
        hidden = gate * jax.nn.sigmoid(gate) * up
        mine[chunk, at, :] = hidden.astype(mine.dtype)

    count = wide.shape[2]
    one = reduce_events(
        order2, places,
        lambda c, b: wide.at[b, c], lambda c, b, at: wide[b, c, at, :], put,
        slots, sums, count, send2, recv2, events,
    )
    lastly = max(at for at, _ in events)
    two = gather_events(
        order, places, lambda c: rows.at[c],
        lambda c, b: full.at[pl.ds(c * span, span), columns(b)],
        send, recv, events, 0.01,
    )
    three = gather_events(
        order3, places, lambda c: mine.at[c], lambda c, b: hid_all.at[b, c],
        send3, recv3, events, lastly + 0.01,
    )
    for c in range(rows.shape[0]):
        full[pl.ds(c * span, span), columns(me)] = rows[c]
    run_events(events, (one, two, three))
    hid_all[me] = mine[...]


def expert_in(rows, wide, half, tp_count):
    sizes = (tp_count // 2, 2)
    order = timed(tp_tree(tp_count, 2), 4.2, 1.0)
    order2 = timed(tp_tree(tp_count, 2), 3.2, 1.0)
    order3 = timed(tp_tree(tp_count, 2), 1.6, 1.0)
    bf16 = rows.dtype
    chunks, span, part = rows.shape
    _, _, count, cols = wide.shape
    return pl.pallas_call(
        functools.partial(expert_in_kernel, order, order2, order3, sizes, half),
        out_shape=(
            jax.ShapeDtypeStruct((chunks * span, part * tp_count), bf16),
            jax.ShapeDtypeStruct((tp_count, 2, count, half), bf16),
        ),
        in_specs=vmem(2),
        out_specs=tuple(vmem(2)),
        scratch_shapes=[
            pltpu.VMEM((2, count, half), bf16),
            pltpu.VMEM((len(order2), count, cols), bf16),
            pltpu.VMEM((len(order2), count, cols), bf16),
        ]
        + dma_sems(order) + dma_sems(order2) + dma_sems(order3),
        compiler_params=params(3),
        name="expert_in",
    )(rows, wide)


def expert_out_kernel(order, sizes, partial, weight, out, slots, sums, send, recv):
    places = Places("tp", sizes)
    places.greet()
    chunks, span, part = out.shape
    events = []

    def columns(b):
        return pl.ds(pl.multiple_of(b * part, part), part)

    def load(c, b, at):
        return partial[c, at, columns(b)]

    def put(c, at, value):
        out[c, at, :] = (value * weight[c, at, :1]).astype(out.dtype)

    one = reduce_events(
        order, places, lambda c, b: partial.at[c, :, columns(b)], load, put,
        slots, sums, span, send, recv, events,
    )
    run_events(events, (one,))


def expert_out(partial, weight, tp_count):
    sizes = (tp_count // 2, 2)
    order = timed(tp_tree(tp_count, 2), 4.2, 1.0)
    chunks, span, width = partial.shape
    part = width // tp_count
    bf16 = partial.dtype
    return pl.pallas_call(
        functools.partial(expert_out_kernel, order, sizes),
        out_shape=jax.ShapeDtypeStruct((chunks, span, part), bf16),
        in_specs=vmem(2),
        out_specs=vmem(1)[0],
        scratch_shapes=[pltpu.VMEM((len(order), span, part), bf16)] * 2 + dma_sems(order),
        compiler_params=params(4),
        name="expert_out",
    )(partial, weight)


def collect_kernel(order, sizes, blocks, resid, out, slots, sums, send, recv):
    places = Places("ep", sizes)
    places.greet()
    events = []

    def put(c, at, value):
        out[c, at, :] = (resid[c, at, :].astype(jnp.float32) + value).astype(out.dtype)

    one = reduce_events(
        order, places, lambda c, b: blocks.at[b, c], lambda c, b, at: blocks[b, c, at, :], put,
        slots, sums, resid.shape[1], send, recv, events,
    )
    run_events(events, (one,))


def collect(blocks, resid, sizes):
    order = timed(ep_tree(sizes), 1.0, 1.8)
    _, _, rows, cols = blocks.shape
    bf16 = blocks.dtype
    return pl.pallas_call(
        functools.partial(collect_kernel, order, sizes),
        out_shape=jax.ShapeDtypeStruct(resid.shape, bf16),
        in_specs=vmem(2),
        out_specs=vmem(1)[0],
        scratch_shapes=[pltpu.VMEM((len(order), rows, cols), bf16)] * 2 + dma_sems(order),
        compiler_params=params(5),
        name="collect",
    )(blocks, resid)


def split_up(x, dim, peers):
    before, after = (x.shape[:dim], x.shape[dim + 1 :])
    return jnp.moveaxis(x.reshape(*before, peers, -1, *after), dim, 0)


def rms_norm(values, gain):
    flt = values.astype(jnp.float32)
    scaled = flt * lax.rsqrt(jnp.mean(flt * flt, axis=-1, keepdims=True) + 1e-06)
    return (scaled * gain).astype(jnp.bfloat16)


def discretize(decay_rate, frequency, log_step, b_real, b_imag):
    step_size = jnp.exp(log_step)[:, None]
    lam_re = -decay_rate
    magnitude = jnp.exp(lam_re * step_size)
    abar_re = magnitude * jnp.cos(frequency * step_size)
    abar_im = magnitude * jnp.sin(frequency * step_size)
    denom = lam_re * lam_re + frequency * frequency
    fac_re = ((abar_re - 1.0) * lam_re + abar_im * frequency) / denom
    fac_im = (abar_im * lam_re - (abar_re - 1.0) * frequency) / denom
    bbar_re = fac_re[..., None] * b_real - fac_im[..., None] * b_imag
    bbar_im = fac_re[..., None] * b_imag + fac_im[..., None] * b_real
    return (abar_re, abar_im, bbar_re, bbar_im)


def state_step(
    drive, states, decay_rate, frequency, log_step, b_real, b_imag, c_real, c_imag, skip_gain
):
    count = drive.shape[0]
    groups = decay_rate.shape[0]
    abar_re, abar_im, bbar_re, bbar_im = discretize(decay_rate, frequency, log_step, b_real, b_imag)
    grouped = drive.astype(jnp.float32).reshape(count, groups, GROUP)
    old_re = states[0].reshape(count, groups, STATE)
    old_im = states[1].reshape(count, groups, STATE)
    push_re = jnp.einsum("ngh,gph->ngp", grouped, bbar_re)
    push_im = jnp.einsum("ngh,gph->ngp", grouped, bbar_im)
    new_re = abar_re * old_re - abar_im * old_im + push_re
    new_im = abar_re * old_im + abar_im * old_re + push_im
    readout = (
        jnp.einsum("ngp,ghp->ngh", new_re, c_real)
        - jnp.einsum("ngp,ghp->ngh", new_im, c_imag)
        + skip_gain.reshape(groups, GROUP) * grouped
    )
    reads = jax.nn.gelu(readout.reshape(count, groups * GROUP)).astype(jnp.bfloat16)
    fresh = jnp.stack(
        [new_re.reshape(count, groups * STATE), new_im.reshape(count, groups * STATE)]
    )
    return (reads, fresh)


def shards(
    tokens,
    mix_gain,
    ffn_gain,
    in_proj,
    decay_rate,
    frequency,
    log_step,
    b_real,
    b_imag,
    c_real,
    c_imag,
    skip_gain,
    states,
    out_proj,
    route_ids,
    route_logits,
    expert_gate,
    expert_up,
    expert_down,
    dense_gate,
    dense_up,
    dense_down,
    branch_gate,
):
    seq_count, width = tokens.shape
    tp_count = lax.axis_size("tp")
    ep_count = lax.axis_size(EP)
    tp_index = lax.axis_index("tp")
    ep_index = lax.axis_index(EP)
    part_width = width // tp_count
    f32, bf16 = jnp.float32, jnp.bfloat16
    top_count = route_ids.shape[1]
    capacity = max(2, 2 * seq_count * top_count // ep_count)
    slots = ep_count * capacity

    route_weights = jax.nn.softmax(route_logits, axis=-1)
    route_rows = jnp.zeros((8, 128), f32)
    route_rows = route_rows.at[1 : 1 + top_count, :seq_count].set(route_ids.astype(f32).T)
    weight_at = 1 + top_count
    route_rows = route_rows.at[weight_at : weight_at + top_count, :seq_count].set(route_weights.T)

    out_cols = lax.all_to_all(split_up(out_proj, 1, tp_count), "tp", 0, 0, tiled=True)
    out_cols = out_cols.reshape(tp_count * out_proj.shape[0], part_width)

    normed = rms_norm(tokens, mix_gain)
    drive = jnp.dot(normed, in_proj, preferred_element_type=f32).astype(bf16)
    reads, new_states = state_step(
        drive, states, decay_rate, frequency, log_step, b_real, b_imag, c_real, c_imag, skip_gain
    )
    token_cols = lax.dynamic_slice_in_dim(tokens, tp_index * part_width, part_width, 1)
    gain_cols = lax.dynamic_slice_in_dim(ffn_gain, tp_index * part_width, part_width, 0)[None]
    gate_cols = lax.dynamic_slice_in_dim(branch_gate, tp_index * part_width, part_width, 0)
    normed_two, resid, branch = mix(
        reads, out_cols, token_cols, gain_cols, gate_cols.astype(f32)[None], route_rows,
        tp_count, width
    )
    sizes = (lax.axis_size("ep_0"), lax.axis_size("ep_1"))
    everyone, branch_all = spread(normed_two, branch, sizes)
    everyone = everyone.reshape(ep_count * seq_count, part_width)
    route_all = branch_all[:, 1:, :seq_count]
    match = (route_all[:, :top_count] == ep_index.astype(f32)).astype(f32)
    named = jnp.sum(match, axis=1)
    weight_all = jnp.sum(match * route_all[:, top_count : 2 * top_count], axis=1).reshape(-1)
    order = jnp.arange(seq_count)
    before = (order[:, None] < order[None, :]).astype(f32)
    slot = jnp.dot(named, before, preferred_element_type=f32)
    place = slot + capacity * jnp.arange(ep_count, dtype=f32)[:, None]
    place = jnp.where(named > 0, place, -1.0).reshape(-1)
    select = place[None, :] == jnp.arange(slots, dtype=f32)[:, None]
    select = select.astype(bf16)
    row_weight = jnp.sum(select.astype(f32) * weight_all[None, :], axis=1)
    branch_all = branch_all[:, 0, :seq_count].reshape(ep_count * seq_count, 1)

    both_proj = jnp.concatenate([dense_gate, dense_up], axis=1)
    hidden_width = dense_gate.shape[1]
    wide = jnp.dot(everyone, both_proj, preferred_element_type=f32).astype(bf16)
    rows_in = jnp.dot(select, everyone, preferred_element_type=f32).astype(bf16)
    full_rows, dense_hidden = expert_in(
        rows_in.reshape(2, slots // 2, part_width),
        wide.reshape(tp_count, 2, -1, 2 * hidden_width),
        hidden_width,
        tp_count,
    )
    dense_hidden = dense_hidden.reshape(ep_count * seq_count, hidden_width)
    gate_val = jnp.dot(full_rows, expert_gate[0], preferred_element_type=f32)
    up_val = jnp.dot(full_rows, expert_up[0], preferred_element_type=f32)
    hidden = (jax.nn.silu(gate_val) * up_val).astype(bf16)
    partial = jnp.dot(hidden, expert_down[0], preferred_element_type=f32).astype(bf16)
    row_weight = jnp.broadcast_to(row_weight[:, None], (slots, 128)).reshape(2, slots // 2, 128)
    weighted = expert_out(partial.reshape(2, slots // 2, width), row_weight, tp_count)
    weighted = weighted.reshape(slots, part_width)

    dense_part = jnp.dot(dense_hidden, dense_down, preferred_element_type=f32)
    routed = lax.dot_general(select, weighted, (((0,), (0,)), ((), ())), preferred_element_type=f32)
    mine = (routed + branch_all * dense_part).astype(bf16)
    output = collect(
        mine.reshape(ep_count, 2, seq_count // 2, part_width),
        resid.reshape(2, seq_count // 2, part_width),
        sizes,
    )
    return (output.reshape(seq_count, part_width), new_states)


def solution(mesh):
    finer = Mesh(mesh.devices.reshape(8, 4, mesh.shape["tp"]), ("ep_0", "ep_1", "tp"))
    return jax.shard_map(
        shards,
        mesh=finer,
        in_specs=(
            P(EP, None),
            P(),
            P(),
            P(None, "tp"),
            P("tp", None),
            P("tp", None),
            P("tp"),
            P("tp", None, None),
            P("tp", None, None),
            P("tp", None, None),
            P("tp", None, None),
            P("tp"),
            P(None, EP, "tp"),
            P("tp", None),
            P(EP, None),
            P(EP, None),
            P(EP, None, "tp"),
            P(EP, None, "tp"),
            P(EP, "tp", None),
            P("tp", EP),
            P("tp", EP),
            P(EP, "tp"),
            P(),
        ),
        out_specs=(P(EP, "tp"), P(None, EP, "tp")),
        check_vma=False,
    )
```

```python
import functools
import heapq

import jax
import jax.numpy as jnp
from jax import lax
from jax.experimental import pallas as pl
from jax.experimental.pallas import tpu as pltpu
from jax.sharding import Mesh
from jax.sharding import PartitionSpec as P

GROUP = 16
STATE = 64
EP = ("ep_0", "ep_1")
MESH = pl.DeviceIdType.MESH
LAG_EP, LAG_TP, LAG_CORE, GAP = 4.0, 7.0, 3.0, 3.4


class Node:
    def __init__(self, chunk, off, parent, move):
        self.chunk, self.off, self.parent, self.move = chunk, off, parent, move
        self.kids = []
        if parent is not None:
            parent.kids.append(self)


def ring_offsets(size, far_up):
    up = size // 2 if far_up else (size - 1) // 2
    return up, size - 1 - up


def chain(chunk, root, axis, name, size, far_up):
    up, down = ring_offsets(size, far_up)
    found = [root]
    for step, count in ((1, up), (-1, down)) if far_up else ((-1, down), (1, up)):
        last = root
        for _ in range(count):
            off = list(last.off)
            off[axis] += step
            last = Node(chunk, tuple(off), last, (name, step))
            found.append(last)
    return found


def ep_tree(sizes):
    nodes = []
    for chunk in range(2):
        first, second = (0, 1) if chunk == 0 else (1, 0)
        root = Node(chunk, (0, 0), None, None)
        line = chain(chunk, root, first, EP[first], sizes[first], True)
        for i, node in enumerate(line):
            nodes += chain(chunk, node, second, EP[second], sizes[second], i % 2 == 0)
    return nodes


def tp_tree(tp_count, chunks, only=None):
    nodes = []
    for chunk in range(chunks) if only is None else only:
        root = Node(chunk, (0, 0), None, None)
        line = chain(chunk, root, 0, "y", tp_count // 2, chunk % 2 == 0)
        for node in line:
            nodes += [node, Node(chunk, (node.off[0], 1), node, ("core", 1))]
    return nodes


def timed(nodes, cost, lag):
    free, heap, order = {}, [], []
    for i, node in enumerate(nodes):
        if node.parent is None:
            node.sent, node.came = 0.0, 0.0
            heapq.heappush(heap, (0.0, i))
    place = {id(node): i for i, node in enumerate(nodes)}
    while heap:
        now, i = heapq.heappop(heap)
        node = nodes[i]
        order.append(node)
        for kid in node.kids:
            price = cost * (0.35 if kid.move[0] == "core" else 1.0)
            start = max(now, free.get(kid.move, 0.0))
            free[kid.move] = start + price
            kid.sent = start
            kid.came = start + price + (LAG_CORE if kid.move[0] == "core" else lag)
            heapq.heappush(heap, (kid.came, place[id(kid)]))
    for i, node in enumerate(order):
        node.index = i
    return order


class Places:
    def __init__(self, kind, sizes):
        self.kind, self.sizes, self.known, self.flats = kind, sizes, {}, {}
        if kind == "ep":
            self.me = (lax.axis_index("ep_0"), lax.axis_index("ep_1"))
        else:
            t = lax.axis_index("tp")
            self.me = (t // 2, t % 2)

    def along(self, axis, off):
        size = self.sizes[axis]
        off = off % size
        if off == 0:
            return self.me[axis]
        if (axis, off) not in self.known:
            self.known[axis, off] = lax.rem(self.me[axis] + off, size)
        return self.known[axis, off]

    def shifted(self, off):
        return tuple(self.along(axis, o) for axis, o in enumerate(off))

    def flat(self, at):
        return at[0] * self.sizes[1] + at[1]

    def owner(self, off):
        return self.at(tuple(-o for o in off))

    def at(self, off):
        key = tuple(o % size for o, size in zip(off, self.sizes))
        if key not in self.flats:
            self.flats[key] = self.flat(self.shifted(key))
        return self.flats[key]

    def device(self, move, sign=1):
        name, step = move
        step = step * sign
        if self.kind == "ep":
            axis = EP.index(name)
            return {name: self.along(axis, step)}
        return {"tp": self.at((step, 0) if name == "y" else (0, step))}

    def greet(self):
        barrier = pltpu.get_barrier_semaphore()
        moves = [("ep_0", 1), ("ep_0", -1), ("ep_1", 1), ("ep_1", -1)]
        if self.kind == "tp":
            moves = [("y", 1), ("y", -1), ("core", 1)]
        for move in moves:
            pl.semaphore_signal(barrier, inc=1, device_id=self.device(move), device_id_type=MESH)
        pl.semaphore_wait(barrier, len(moves))


def gather_events(order, places, source, target, send, recv, events, base=0.0):
    started = []

    def copy(node, src, device):
        own = places.owner(node.parent.off) if node.parent is not None else None
        return pltpu.make_async_remote_copy(
            src_ref=src,
            dst_ref=target(node.chunk, own),
            send_sem=send.at[node.index],
            recv_sem=recv.at[node.index],
            device_id=device,
            device_id_type=MESH,
        )

    def handle(node):
        if node.parent is None:
            src = source(node.chunk)
        else:
            src = target(node.chunk, places.owner(node.off))
            pltpu.make_async_remote_copy(
                src_ref=src,
                dst_ref=src,
                send_sem=send.at[node.index],
                recv_sem=recv.at[node.index],
                device_id=places.device(node.move),
                device_id_type=MESH,
            ).wait_recv()
        for kid in node.kids:
            moved = copy(kid, src, places.device(kid.move))
            moved.start()
            started.append(moved)

    for node in order:
        events.append((base + node.came, functools.partial(handle, node)))
    return started


def add_into(out, terms, rows, step=48):
    def body(i):
        at = pl.ds(i * step, step)
        total = terms[0](at).astype(jnp.float32)
        for term in terms[1:]:
            total = total + term(at).astype(jnp.float32)
        out(at, total)

    for i in range(rows // step):
        body(i)


def reduce_events(order, places, view, load, put, slots, sums, rows, send, recv, events, base=0.0):
    started = []
    last = max(node.came for node in order)

    def handle(node):
        off = node.off
        own = places.owner(off)
        for kid in node.kids:
            slot = slots.at[kid.index]
            pltpu.make_async_remote_copy(
                src_ref=slot,
                dst_ref=slot,
                send_sem=send.at[kid.index],
                recv_sem=recv.at[kid.index],
                device_id=places.device(kid.move),
                device_id_type=MESH,
            ).wait_recv()
        terms = [lambda at: load(node.chunk, own, at)]
        for kid in node.kids:
            terms.append(lambda at, k=kid.index: slots[k, at, :])
        if node.parent is None:
            add_into(lambda at, v: put(node.chunk, at, v), terms, rows)
            return
        if node.kids:
            src = sums.at[node.index]

            def keep(at, v):
                sums[node.index, at, :] = v.astype(sums.dtype)

            add_into(keep, terms, rows)
        else:
            src = view(node.chunk, own)
        moved = pltpu.make_async_remote_copy(
            src_ref=src,
            dst_ref=slots.at[node.index],
            send_sem=send.at[node.index],
            recv_sem=recv.at[node.index],
            device_id=places.device(node.move, -1),
            device_id_type=MESH,
        )
        moved.start()
        started.append(moved)

    for node in reversed(order):
        events.append((base + last - node.came, functools.partial(handle, node)))
    return started


def run_events(events, started):
    for _, act in sorted(events, key=lambda pair: pair[0]):
        act()
    for group in started:
        for moved in group:
            moved.wait_send()


def vmem(count):
    return [pl.BlockSpec(memory_space=pltpu.VMEM)] * count


def dma_sems(order):
    return [pltpu.SemaphoreType.DMA((len(order),))] * 2


def params(collective_id):
    return pltpu.CompilerParams(collective_id=collective_id, has_side_effects=True)


def mix_kernel(
    tp_count, width, reads, weights, tokens, gain, gate, route,
    normed, resid, branch, held, stats, send, recv, send2, recv2,
):
    me = lax.axis_index("tp")
    barrier = pltpu.get_barrier_semaphore()
    others = [lax.rem(me + k, tp_count) for k in range(1, tp_count)]
    for other in others:
        pl.semaphore_signal(barrier, inc=1, device_id={"tp": other}, device_id_type=MESH)
    pl.semaphore_wait(barrier, tp_count - 1)

    def exchange(src, dst, send, recv):
        copies = []
        for k, other in enumerate(others):
            copies.append(
                pltpu.make_async_remote_copy(
                    src_ref=src,
                    dst_ref=dst.at[k + 1],
                    send_sem=send.at[k],
                    recv_sem=recv.at[k],
                    device_id={"tp": other},
                    device_id_type=MESH,
                )
            )
            copies[-1].start()
        return copies

    copies = exchange(reads, held, send, recv)
    depth = reads.shape[1]
    f32 = jnp.float32

    def part(value, k):
        owner = lax.rem(me + tp_count - k, tp_count)
        at = pl.ds(pl.multiple_of(owner * depth, depth), depth)
        return jnp.dot(value, weights[at, :], preferred_element_type=f32)

    total = part(reads[...], 0)
    for k, copy in enumerate(copies):
        copy.wait()
        total = total + part(held[k + 1], k + 1)
    flt = tokens[...].astype(f32) + total.astype(jnp.bfloat16).astype(f32)
    flt = flt.astype(jnp.bfloat16).astype(f32)
    resid[...] = flt.astype(jnp.bfloat16)
    gained = flt * gain[...]
    ones = jnp.ones((8, flt.shape[1]), f32)
    high = lax.Precision.HIGHEST
    turned = (((1,), (1,)), ((), ()))
    square = lax.dot_general(ones, flt * flt, turned, precision=high, preferred_element_type=f32)
    logit = lax.dot_general(
        ones, gained * gate[...], turned, precision=high, preferred_element_type=f32
    )
    rows = flt.shape[0]
    stats[0, 0, :, :rows] = square
    stats[0, 1, :, :rows] = logit
    copies = exchange(stats.at[0], stats, send2, recv2)
    for copy in copies:
        copy.wait()
    both = stats[0]
    for k in range(1, tp_count):
        both = both + stats[k]
    scale = lax.rsqrt(both[0, :, :rows] / width + 1e-06)
    branch[...] = route[...]
    branch[:1, :rows] = jax.nn.sigmoid(scale * both[1, :, :rows])[:1]
    first = (lax.broadcasted_iota(jnp.int32, (8, flt.shape[1]), 0) == 0).astype(f32)
    column = lax.dot_general(
        scale, first, (((0,), (0,)), ((), ())), precision=high, preferred_element_type=f32
    )
    value = (gained * column).astype(jnp.bfloat16)
    half = rows // 2
    normed[0] = value[:half]
    normed[1] = value[half:]


def mix(reads, weights, tokens, gain, gate, route, tp_count, width):
    rows, cols = tokens.shape
    bf16, f32 = jnp.bfloat16, jnp.float32
    return pl.pallas_call(
        functools.partial(mix_kernel, tp_count, width),
        out_shape=(
            jax.ShapeDtypeStruct((2, rows // 2, cols), bf16),
            jax.ShapeDtypeStruct((rows, cols), bf16),
            jax.ShapeDtypeStruct((8, 128), f32),
        ),
        in_specs=vmem(6),
        out_specs=tuple(vmem(3)),
        scratch_shapes=[
            pltpu.VMEM((tp_count, *reads.shape), bf16),
            pltpu.VMEM((tp_count, 2, 8, 128), f32),
        ]
        + [pltpu.SemaphoreType.DMA((tp_count - 1,))] * 4,
        compiler_params=params(1),
        name="mix",
    )(reads, weights, tokens, gain, gate, route)


def forward_plan(sizes, tp_count):
    big = timed(ep_tree(sizes), 1.06, LAG_EP)
    small = timed([n for n in ep_tree(sizes) if n.chunk == 0], 0.1, LAG_EP)
    ready = {}
    for node in big + small:
        dz = node.off[0] % sizes[0]
        ready[dz] = max(ready.get(dz, 0.0), node.came)
    ranks, base = [], 0.0
    for dz in sorted(ready, key=lambda d: ready[d]):
        base = max(ready[dz] + 1.0, base + GAP)
        ranks.append((dz, base))
    flows = []
    for rank, (dz, base) in enumerate(ranks):
        trees = [timed(tp_tree(tp_count, 2, (rank % 2,)), cost, LAG_TP) for cost in (1.06, 0.8, 0.4)]
        flows.append((dz, base, trees))
    return big, small, flows


def forward_kernel(
    big, small, flows, sizes, tp_sizes, capacity,
    block, extra, both, gate_hbm, up_hbm, down_hbm,
    partial, hid_all, extra_all,
    out, wide, rows, full, mine, slots, sums, gate_w, up_w, down_w, gate_val, hidden,
    send, recv, send2, recv2, send3, recv3, send4, recv4, send5, recv5, loaded,
):
    f32, bf16 = jnp.float32, jnp.bfloat16
    loads = [
        pltpu.make_async_copy(src, dst, loaded.at[i])
        for i, (src, dst) in enumerate(((gate_hbm, gate_w), (up_hbm, up_w), (down_hbm, down_w)))
    ]
    for load in loads:
        load.start()
    places, tp = Places("ep", sizes), Places("tp", tp_sizes)
    barrier = pltpu.get_barrier_semaphore()
    for name in EP:
        for step in (1, -1):
            device = places.device((name, step))
            pl.semaphore_signal(barrier, inc=1, device_id=device, device_id_type=MESH)
    for move in (("y", 1), ("y", -1), ("core", 1)):
        pl.semaphore_signal(barrier, inc=1, device_id=tp.device(move), device_id_type=MESH)
    pl.semaphore_wait(barrier, 7)

    mine_at = places.flat(places.me)
    expert = mine_at.astype(f32)
    me = tp.flat(tp.me)
    zs, xs = sizes
    _, half_rows, part = block.shape
    seq = 2 * half_rows
    span = capacity * xs
    half = hidden.shape[1]
    hid = both.shape[1] // 2
    mine[...] = jnp.zeros_like(mine)
    events, started = [], []
    out[mine_at] = block[...]
    extra_all[mine_at] = extra[...]
    started.append(
        gather_events(
            big, places, lambda c: block.at[c], lambda c, b: out.at[b, c], send, recv, events
        )
    )
    started.append(
        gather_events(
            small, places, lambda c: extra, lambda c, b: extra_all.at[b], send2, recv2, events, 0.1
        )
    )
    lane = lax.broadcasted_iota(jnp.int32, (8, 128), 1)
    before = lax.broadcasted_iota(jnp.int32, (128, 128), 0) < lax.broadcasted_iota(
        jnp.int32, (128, 128), 1
    )
    before = before.astype(f32)
    slot_at = lax.broadcasted_iota(jnp.int32, (span, 128), 0).astype(f32)

    def columns(b):
        return pl.ds(pl.multiple_of(b * part, part), part)

    def use_group(rank, dz):
        first = pl.multiple_of(places.along(0, -dz) * xs, xs)
        picked = jnp.zeros((span, part), f32)
        for x in range(xs):
            info = extra_all[first + x]
            named = (info[1:2] == expert) | (info[2:3] == expert)
            named = jnp.where(named & (lane[:1] < seq), 1.0, 0.0)
            slot = jnp.dot(
                jnp.broadcast_to(named, (8, 128)), before, preferred_element_type=f32
            )[:1]
            place = jnp.where(named > 0, slot + float(capacity * x), -1.0)
            select = jnp.where(place == slot_at, 1.0, 0.0)[:, :seq].astype(bf16)
            value = out[first + x].reshape(seq, part)
            picked = picked + jnp.dot(select, value, preferred_element_type=f32)
        rows[rank] = picked.astype(bf16)
        full[pl.ds(rank * span, span), columns(me)] = picked.astype(bf16)
        value = out[pl.ds(first, xs)].reshape(xs * seq, part)
        product = jnp.dot(value, both[...], preferred_element_type=f32).astype(bf16)
        wide[rank] = product.reshape(2 * xs, half_rows, product.shape[1])

    nodes = len(flows[0][2][0])
    row_time = []
    for rank, (dz, base, (row_tree, sum_tree, hid_tree)) in enumerate(flows):
        events.append((base - 0.1, functools.partial(use_group, rank, dz)))
        sems = [
            sem.at[pl.ds(rank * nodes, nodes)] for sem in (send3, recv3, send4, recv4, send5, recv5)
        ]

        def put(chunk, at, value, rank=rank):
            gate, up = value[:, :hid], value[:, hid:]
            mine[rank, at, :hid] = (gate * jax.nn.sigmoid(gate) * up).astype(bf16)

        started.append(
            reduce_events(
                sum_tree, tp,
                lambda c, b, r=rank: wide.at[r, b],
                lambda c, b, at, r=rank: wide[r, b, at, :],
                put, slots.at[rank], sums.at[rank], half_rows, sems[2], sems[3], events, base,
            )
        )
        summed = base + max(node.came for node in sum_tree)
        started.append(
            gather_events(
                row_tree, tp,
                lambda c, r=rank: rows.at[r],
                lambda c, b, r=rank: full.at[pl.ds(r * span, span), columns(b)],
                sems[0], sems[1], events, base + 0.01,
            )
        )
        row_time.append(base + 0.01 + max(node.came for node in row_tree))

        def keep(rank, dz):
            hid_all[places.along(0, -dz), me] = mine[rank]

        events.append((summed + 0.01, functools.partial(keep, rank, dz)))

        def hid_target(c, b, dz=dz):
            return hid_all.at[places.along(0, -dz), b]

        started.append(
            gather_events(
                hid_tree, tp, lambda c, r=rank: mine.at[r], hid_target,
                sems[4], sems[5], events, summed + 0.02,
            )
        )

    group_rows = full.shape[0] // 2

    def gate_part(h):
        if h == 0:
            loads[0].wait()
        value = full[pl.ds(h * group_rows, group_rows), :]
        gate_val[...] = jnp.dot(value, gate_w[...], preferred_element_type=f32)

    def up_part(h):
        if h == 0:
            loads[1].wait()
        value = full[pl.ds(h * group_rows, group_rows), :]
        up_val = jnp.dot(value, up_w[...], preferred_element_type=f32)
        gate = gate_val[...]
        hidden[...] = (gate * jax.nn.sigmoid(gate) * up_val).astype(bf16)

    def down_part(h, piece, pieces):
        if h == 0 and piece == 0:
            loads[2].wait()
        width = partial.shape[2] // pieces
        at = slice(piece * width, (piece + 1) * width)
        product = jnp.dot(hidden[...], down_w[:, at], preferred_element_type=f32)
        partial[h, :, at] = product.astype(bf16)

    for h in range(2):
        when = max(row_time[h * len(flows) // 2 : (h + 1) * len(flows) // 2]) + 0.02
        if h == 1:
            when = max(when, max(at for at, _ in events) + 0.02)
        step = 1.5
        events.append((when, functools.partial(gate_part, h)))
        events.append((when + step, functools.partial(up_part, h)))
        for piece in range(4):
            act = functools.partial(down_part, h, piece, 4)
            events.append((when + step * 2 + piece * step / 2, act))
    run_events(events, started)


def forward(block, extra, both, gate_w, up_w, down_w, sizes, tp_count, capacity):
    count = sizes[0] * sizes[1]
    tp_sizes = (tp_count // 2, 2)
    big, small, flows = forward_plan(sizes, tp_count)
    bf16, f32 = block.dtype, jnp.float32
    _, half_rows, part = block.shape
    span = capacity * sizes[1]
    slots = capacity * count
    width = part * tp_count
    half = gate_w.shape[1]
    hid = both.shape[1] // 2
    lanes = -(-hid // 128) * 128
    groups = sizes[0]
    nodes = groups * len(flows[0][2][0])
    anywhere = [pl.BlockSpec(memory_space=pl.ANY)] * 3
    return pl.pallas_call(
        functools.partial(forward_kernel, big, small, flows, sizes, tp_sizes, capacity),
        out_shape=(
            jax.ShapeDtypeStruct((2, slots // 2, width), bf16),
            jax.ShapeDtypeStruct((groups, tp_count, half_rows, lanes), bf16),
            jax.ShapeDtypeStruct((count, *extra.shape), f32),
        ),
        in_specs=vmem(3) + anywhere,
        out_specs=tuple(vmem(3)),
        scratch_shapes=[
            pltpu.VMEM((count, 2, half_rows, part), bf16),
            pltpu.VMEM((groups, tp_count, half_rows, 2 * hid), bf16),
            pltpu.VMEM((groups, span, part), bf16),
            pltpu.VMEM((slots, width), bf16),
            pltpu.VMEM((groups, half_rows, lanes), bf16),
            pltpu.VMEM((groups, nodes // groups, half_rows, 2 * hid), bf16),
            pltpu.VMEM((groups, nodes // groups, half_rows, 2 * hid), bf16),
            pltpu.VMEM(gate_w.shape, bf16),
            pltpu.VMEM(up_w.shape, bf16),
            pltpu.VMEM(down_w.shape, bf16),
            pltpu.VMEM((slots // 2, half), f32),
            pltpu.VMEM((slots // 2, half), bf16),
        ]
        + dma_sems(big)
        + dma_sems(small)
        + [pltpu.SemaphoreType.DMA((nodes,))] * 6
        + [pltpu.SemaphoreType.DMA((3,))],
        compiler_params=params(2),
        name="forward",
    )(block, extra, both, gate_w, up_w, down_w)


def expert_out_kernel(order, sizes, partial, weight, out, slots, sums, send, recv):
    places = Places("tp", sizes)
    places.greet()
    chunks, span, part = out.shape
    events = []

    def columns(b):
        return pl.ds(pl.multiple_of(b * part, part), part)

    def load(c, b, at):
        return partial[c, at, columns(b)]

    def put(c, at, value):
        out[c, at, :] = (value * weight[c, at, :1]).astype(out.dtype)

    one = reduce_events(
        order, places, lambda c, b: partial.at[c, :, columns(b)], load, put,
        slots, sums, span, send, recv, events,
    )
    run_events(events, (one,))


def expert_out(partial, weight, tp_count):
    sizes = (tp_count // 2, 2)
    order = timed(tp_tree(tp_count, 2), 4.2, LAG_TP)
    chunks, span, width = partial.shape
    part = width // tp_count
    bf16 = partial.dtype
    return pl.pallas_call(
        functools.partial(expert_out_kernel, order, sizes),
        out_shape=jax.ShapeDtypeStruct((chunks, span, part), bf16),
        in_specs=vmem(2),
        out_specs=vmem(1)[0],
        scratch_shapes=[pltpu.VMEM((len(order), span, part), bf16)] * 2 + dma_sems(order),
        compiler_params=params(4),
        name="expert_out",
    )(partial, weight)


def collect_kernel(order, sizes, blocks, resid, out, slots, sums, send, recv):
    places = Places("ep", sizes)
    places.greet()
    events = []

    def put(c, at, value):
        out[c, at, :] = (resid[c, at, :].astype(jnp.float32) + value).astype(out.dtype)

    one = reduce_events(
        order, places, lambda c, b: blocks.at[b, c], lambda c, b, at: blocks[b, c, at, :], put,
        slots, sums, resid.shape[1], send, recv, events,
    )
    run_events(events, (one,))


def collect(blocks, resid, sizes):
    order = timed(ep_tree(sizes), 1.06, LAG_EP)
    _, _, rows, cols = blocks.shape
    bf16 = blocks.dtype
    return pl.pallas_call(
        functools.partial(collect_kernel, order, sizes),
        out_shape=jax.ShapeDtypeStruct(resid.shape, bf16),
        in_specs=vmem(2),
        out_specs=vmem(1)[0],
        scratch_shapes=[pltpu.VMEM((len(order), rows, cols), bf16)] * 2 + dma_sems(order),
        compiler_params=params(5),
        name="collect",
    )(blocks, resid)


def split_up(x, dim, peers):
    before, after = (x.shape[:dim], x.shape[dim + 1 :])
    return jnp.moveaxis(x.reshape(*before, peers, -1, *after), dim, 0)


def rms_norm(values, gain):
    flt = values.astype(jnp.float32)
    scaled = flt * lax.rsqrt(jnp.mean(flt * flt, axis=-1, keepdims=True) + 1e-06)
    return (scaled * gain).astype(jnp.bfloat16)


def discretize(decay_rate, frequency, log_step, b_real, b_imag):
    step_size = jnp.exp(log_step)[:, None]
    lam_re = -decay_rate
    magnitude = jnp.exp(lam_re * step_size)
    abar_re = magnitude * jnp.cos(frequency * step_size)
    abar_im = magnitude * jnp.sin(frequency * step_size)
    denom = lam_re * lam_re + frequency * frequency
    fac_re = ((abar_re - 1.0) * lam_re + abar_im * frequency) / denom
    fac_im = (abar_im * lam_re - (abar_re - 1.0) * frequency) / denom
    bbar_re = fac_re[..., None] * b_real - fac_im[..., None] * b_imag
    bbar_im = fac_re[..., None] * b_imag + fac_im[..., None] * b_real
    return (abar_re, abar_im, bbar_re, bbar_im)


def state_step(
    drive, states, decay_rate, frequency, log_step, b_real, b_imag, c_real, c_imag, skip_gain
):
    count = drive.shape[0]
    groups = decay_rate.shape[0]
    abar_re, abar_im, bbar_re, bbar_im = discretize(decay_rate, frequency, log_step, b_real, b_imag)
    grouped = drive.astype(jnp.float32).reshape(count, groups, GROUP)
    old_re = states[0].reshape(count, groups, STATE)
    old_im = states[1].reshape(count, groups, STATE)
    push_re = jnp.einsum("ngh,gph->ngp", grouped, bbar_re)
    push_im = jnp.einsum("ngh,gph->ngp", grouped, bbar_im)
    new_re = abar_re * old_re - abar_im * old_im + push_re
    new_im = abar_re * old_im + abar_im * old_re + push_im
    readout = (
        jnp.einsum("ngp,ghp->ngh", new_re, c_real)
        - jnp.einsum("ngp,ghp->ngh", new_im, c_imag)
        + skip_gain.reshape(groups, GROUP) * grouped
    )
    reads = jax.nn.gelu(readout.reshape(count, groups * GROUP)).astype(jnp.bfloat16)
    fresh = jnp.stack(
        [new_re.reshape(count, groups * STATE), new_im.reshape(count, groups * STATE)]
    )
    return (reads, fresh)


def shards(
    tokens,
    mix_gain,
    ffn_gain,
    in_proj,
    decay_rate,
    frequency,
    log_step,
    b_real,
    b_imag,
    c_real,
    c_imag,
    skip_gain,
    states,
    out_proj,
    route_ids,
    route_logits,
    expert_gate,
    expert_up,
    expert_down,
    dense_gate,
    dense_up,
    dense_down,
    branch_gate,
):
    seq_count, width = tokens.shape
    tp_count = lax.axis_size("tp")
    ep_count = lax.axis_size(EP)
    tp_index = lax.axis_index("tp")
    ep_index = lax.axis_index(EP)
    part_width = width // tp_count
    f32, bf16 = jnp.float32, jnp.bfloat16
    top_count = route_ids.shape[1]
    capacity = max(2, 2 * seq_count * top_count // ep_count)
    slots = ep_count * capacity

    route_weights = jax.nn.softmax(route_logits, axis=-1)
    route_rows = jnp.zeros((8, 128), f32)
    route_rows = route_rows.at[1 : 1 + top_count, :seq_count].set(route_ids.astype(f32).T)
    weight_at = 1 + top_count
    route_rows = route_rows.at[weight_at : weight_at + top_count, :seq_count].set(route_weights.T)

    out_cols = lax.all_to_all(split_up(out_proj, 1, tp_count), "tp", 0, 0, tiled=True)
    out_cols = out_cols.reshape(tp_count * out_proj.shape[0], part_width)

    normed = rms_norm(tokens, mix_gain)
    drive = jnp.dot(normed, in_proj, preferred_element_type=f32).astype(bf16)
    reads, new_states = state_step(
        drive, states, decay_rate, frequency, log_step, b_real, b_imag, c_real, c_imag, skip_gain
    )
    token_cols = lax.dynamic_slice_in_dim(tokens, tp_index * part_width, part_width, 1)
    gain_cols = lax.dynamic_slice_in_dim(ffn_gain, tp_index * part_width, part_width, 0)[None]
    gate_cols = lax.dynamic_slice_in_dim(branch_gate, tp_index * part_width, part_width, 0)
    normed_two, resid, branch = mix(
        reads, out_cols, token_cols, gain_cols, gate_cols.astype(f32)[None], route_rows,
        tp_count, width
    )
    sizes = (lax.axis_size("ep_0"), lax.axis_size("ep_1"))
    both_proj = jnp.concatenate([dense_gate, dense_up], axis=1)
    partial, dense_hidden, branch_all = forward(
        normed_two, branch, both_proj, expert_gate[0], expert_up[0], expert_down[0],
        sizes, tp_count, capacity,
    )
    dense_hidden = dense_hidden.reshape(ep_count * seq_count, -1)
    spare = dense_hidden.shape[1] - dense_down.shape[0]
    dense_down = jnp.pad(dense_down, ((0, spare), (0, 0)))
    route_all = branch_all[:, 1:, :seq_count]
    match = (route_all[:, :top_count] == ep_index.astype(f32)).astype(f32)
    named = jnp.sum(match, axis=1)
    weight_all = jnp.sum(match * route_all[:, top_count : 2 * top_count], axis=1).reshape(-1)
    order = jnp.arange(seq_count)
    before = (order[:, None] < order[None, :]).astype(f32)
    slot = jnp.dot(named, before, preferred_element_type=f32)
    group = jnp.arange(ep_count, dtype=jnp.int32) // sizes[1]
    offset = lax.rem(lax.axis_index("ep_0") - group + sizes[0], sizes[0])
    rank = jnp.zeros((ep_count,), f32)
    for at, (dz, _, _) in enumerate(forward_plan(sizes, tp_count)[2]):
        rank = jnp.where(offset == dz % sizes[0], float(at), rank)
    within = (jnp.arange(ep_count, dtype=jnp.int32) % sizes[1]).astype(f32)
    place = slot + capacity * (rank * sizes[1] + within)[:, None]
    place = jnp.where(named > 0, place, -1.0).reshape(-1)
    select = place[None, :] == jnp.arange(slots, dtype=f32)[:, None]
    select = select.astype(bf16)
    row_weight = jnp.sum(select.astype(f32) * weight_all[None, :], axis=1)
    branch_all = branch_all[:, 0, :seq_count].reshape(ep_count * seq_count, 1)

    row_weight = jnp.broadcast_to(row_weight[:, None], (slots, 128)).reshape(2, slots // 2, 128)
    weighted = expert_out(partial, row_weight, tp_count)
    weighted = weighted.reshape(slots, part_width)

    dense_part = jnp.dot(dense_hidden, dense_down, preferred_element_type=f32)
    routed = lax.dot_general(select, weighted, (((0,), (0,)), ((), ())), preferred_element_type=f32)
    mine = (routed + branch_all * dense_part).astype(bf16)
    output = collect(
        mine.reshape(ep_count, 2, seq_count // 2, part_width),
        resid.reshape(2, seq_count // 2, part_width),
        sizes,
    )
    return (output.reshape(seq_count, part_width), new_states)


def solution(mesh):
    finer = Mesh(mesh.devices.reshape(8, 4, mesh.shape["tp"]), ("ep_0", "ep_1", "tp"))
    return jax.shard_map(
        shards,
        mesh=finer,
        in_specs=(
            P(EP, None),
            P(),
            P(),
            P(None, "tp"),
            P("tp", None),
            P("tp", None),
            P("tp"),
            P("tp", None, None),
            P("tp", None, None),
            P("tp", None, None),
            P("tp", None, None),
            P("tp"),
            P(None, EP, "tp"),
            P("tp", None),
            P(EP, None),
            P(EP, None),
            P(EP, None, "tp"),
            P(EP, None, "tp"),
            P(EP, "tp", None),
            P("tp", EP),
            P("tp", EP),
            P(EP, "tp"),
            P(),
        ),
        out_specs=(P(EP, "tp"), P(None, EP, "tp")),
        check_vma=False,
    )
```

```python
import functools
import heapq

import jax
import jax.numpy as jnp
from jax import lax
from jax.experimental import pallas as pl
from jax.experimental.pallas import tpu as pltpu
from jax.sharding import Mesh
from jax.sharding import PartitionSpec as P

GROUP = 16
STATE = 64
EP = ("ep_0", "ep_1")
MESH = pl.DeviceIdType.MESH
LAG_EP, LAG_TP, LAG_CORE, LAG_BACK, GAP = 4.0, 7.0, 3.0, 4.0, 3.4


class Node:
    def __init__(self, chunk, off, parent, move):
        self.chunk, self.off, self.parent, self.move = chunk, off, parent, move
        self.kids = []
        if parent is not None:
            parent.kids.append(self)


def ring_offsets(size, far_up):
    up = size // 2 if far_up else (size - 1) // 2
    return up, size - 1 - up


def chain(chunk, root, axis, name, size, far_up):
    up, down = ring_offsets(size, far_up)
    found = [root]
    for step, count in ((1, up), (-1, down)) if far_up else ((-1, down), (1, up)):
        last = root
        for _ in range(count):
            off = list(last.off)
            off[axis] += step
            last = Node(chunk, tuple(off), last, (name, step))
            found.append(last)
    return found


def ep_tree(sizes):
    nodes = []
    for chunk in range(2):
        first, second = (0, 1) if chunk == 0 else (1, 0)
        root = Node(chunk, (0, 0), None, None)
        line = chain(chunk, root, first, EP[first], sizes[first], True)
        for i, node in enumerate(line):
            nodes += chain(chunk, node, second, EP[second], sizes[second], i % 2 == 0)
    return nodes


def tp_tree(tp_count, chunks, only=None):
    nodes = []
    for chunk in range(chunks) if only is None else only:
        root = Node(chunk, (0, 0), None, None)
        line = chain(chunk, root, 0, "y", tp_count // 2, chunk % 2 == 0)
        for node in line:
            nodes += [node, Node(chunk, (node.off[0], 1), node, ("core", 1))]
    return nodes


def timed(nodes, cost, lag):
    free, heap, order = {}, [], []
    for i, node in enumerate(nodes):
        if node.parent is None:
            node.sent, node.came = 0.0, 0.0
            heapq.heappush(heap, (0.0, i))
    place = {id(node): i for i, node in enumerate(nodes)}
    while heap:
        now, i = heapq.heappop(heap)
        node = nodes[i]
        order.append(node)
        for kid in node.kids:
            price = cost * (0.35 if kid.move[0] == "core" else 1.0)
            start = max(now, free.get(kid.move, 0.0))
            free[kid.move] = start + price
            kid.sent = start
            kid.came = start + price + (LAG_CORE if kid.move[0] == "core" else lag)
            heapq.heappush(heap, (kid.came, place[id(kid)]))
    for i, node in enumerate(order):
        node.index = i
    return order


class Places:
    def __init__(self, kind, sizes):
        self.kind, self.sizes, self.known, self.flats = kind, sizes, {}, {}
        if kind == "ep":
            self.me = (lax.axis_index("ep_0"), lax.axis_index("ep_1"))
        else:
            t = lax.axis_index("tp")
            self.me = (t // 2, t % 2)

    def along(self, axis, off):
        size = self.sizes[axis]
        off = off % size
        if off == 0:
            return self.me[axis]
        if (axis, off) not in self.known:
            self.known[axis, off] = lax.rem(self.me[axis] + off, size)
        return self.known[axis, off]

    def shifted(self, off):
        return tuple(self.along(axis, o) for axis, o in enumerate(off))

    def flat(self, at):
        return at[0] * self.sizes[1] + at[1]

    def owner(self, off):
        return self.at(tuple(-o for o in off))

    def at(self, off):
        key = tuple(o % size for o, size in zip(off, self.sizes))
        if key not in self.flats:
            self.flats[key] = self.flat(self.shifted(key))
        return self.flats[key]

    def device(self, move, sign=1):
        name, step = move
        step = step * sign
        if self.kind == "ep":
            axis = EP.index(name)
            return {name: self.along(axis, step)}
        return {"tp": self.at((step, 0) if name == "y" else (0, step))}

    def greet(self):
        barrier = pltpu.get_barrier_semaphore()
        moves = [("ep_0", 1), ("ep_0", -1), ("ep_1", 1), ("ep_1", -1)]
        if self.kind == "tp":
            moves = [("y", 1), ("y", -1), ("core", 1)]
        for move in moves:
            pl.semaphore_signal(barrier, inc=1, device_id=self.device(move), device_id_type=MESH)
        pl.semaphore_wait(barrier, len(moves))


def gather_events(order, places, source, target, send, recv, events, base=0.0):
    started = []

    def copy(node, src, device):
        own = places.owner(node.parent.off) if node.parent is not None else None
        return pltpu.make_async_remote_copy(
            src_ref=src,
            dst_ref=target(node.chunk, own),
            send_sem=send.at[node.index],
            recv_sem=recv.at[node.index],
            device_id=device,
            device_id_type=MESH,
        )

    def handle(node):
        if node.parent is None:
            src = source(node.chunk)
        else:
            src = target(node.chunk, places.owner(node.off))
            pltpu.make_async_remote_copy(
                src_ref=src,
                dst_ref=src,
                send_sem=send.at[node.index],
                recv_sem=recv.at[node.index],
                device_id=places.device(node.move),
                device_id_type=MESH,
            ).wait_recv()
        for kid in node.kids:
            moved = copy(kid, src, places.device(kid.move))
            moved.start()
            started.append(moved)

    for node in order:
        events.append((base + node.came, functools.partial(handle, node)))
    return started


def add_into(out, terms, rows, step=48):
    def body(i):
        at = pl.ds(i * step, step)
        total = terms[0](at).astype(jnp.float32)
        for term in terms[1:]:
            total = total + term(at).astype(jnp.float32)
        out(at, total)

    for i in range(rows // step):
        body(i)


def reduce_events(order, places, view, load, put, slots, sums, rows, send, recv, events, base=0.0):
    started = []
    last = max(node.came for node in order)

    def handle(node):
        off = node.off
        own = places.owner(off)
        for kid in node.kids:
            slot = slots.at[kid.index]
            pltpu.make_async_remote_copy(
                src_ref=slot,
                dst_ref=slot,
                send_sem=send.at[kid.index],
                recv_sem=recv.at[kid.index],
                device_id=places.device(kid.move),
                device_id_type=MESH,
            ).wait_recv()
        terms = [lambda at: load(node.chunk, own, at)]
        for kid in node.kids:
            terms.append(lambda at, k=kid.index: slots[k, at, :])
        if node.parent is None:
            add_into(lambda at, v: put(node.chunk, at, v), terms, rows)
            return
        if node.kids:
            src = sums.at[node.index]

            def keep(at, v):
                sums[node.index, at, :] = v.astype(sums.dtype)

            add_into(keep, terms, rows)
        else:
            src = view(node.chunk, own)
        moved = pltpu.make_async_remote_copy(
            src_ref=src,
            dst_ref=slots.at[node.index],
            send_sem=send.at[node.index],
            recv_sem=recv.at[node.index],
            device_id=places.device(node.move, -1),
            device_id_type=MESH,
        )
        moved.start()
        started.append(moved)

    for node in reversed(order):
        events.append((base + last - node.came, functools.partial(handle, node)))
    return started


def run_events(events, started):
    for _, act in sorted(events, key=lambda pair: pair[0]):
        act()
    for group in started:
        for moved in group:
            moved.wait_send()


def vmem(count):
    return [pl.BlockSpec(memory_space=pltpu.VMEM)] * count


def dma_sems(order):
    return [pltpu.SemaphoreType.DMA((len(order),))] * 2


def params(collective_id):
    return pltpu.CompilerParams(collective_id=collective_id, has_side_effects=True)


def mix_kernel(
    tp_count, width, reads, weights, tokens, gain, gate, route,
    normed, resid, branch, held, stats, send, recv, send2, recv2,
):
    me = lax.axis_index("tp")
    barrier = pltpu.get_barrier_semaphore()
    others = [lax.rem(me + k, tp_count) for k in range(1, tp_count)]
    for other in others:
        pl.semaphore_signal(barrier, inc=1, device_id={"tp": other}, device_id_type=MESH)
    pl.semaphore_wait(barrier, tp_count - 1)

    def exchange(src, dst, send, recv):
        copies = []
        for k, other in enumerate(others):
            copies.append(
                pltpu.make_async_remote_copy(
                    src_ref=src,
                    dst_ref=dst.at[k + 1],
                    send_sem=send.at[k],
                    recv_sem=recv.at[k],
                    device_id={"tp": other},
                    device_id_type=MESH,
                )
            )
            copies[-1].start()
        return copies

    copies = exchange(reads, held, send, recv)
    depth = reads.shape[1]
    f32 = jnp.float32

    def part(value, k):
        owner = lax.rem(me + tp_count - k, tp_count)
        at = pl.ds(pl.multiple_of(owner * depth, depth), depth)
        return jnp.dot(value, weights[at, :], preferred_element_type=f32)

    total = part(reads[...], 0)
    for k, copy in enumerate(copies):
        copy.wait()
        total = total + part(held[k + 1], k + 1)
    cols = pl.ds(pl.multiple_of(me * resid.shape[1], resid.shape[1]), resid.shape[1])
    flt = tokens[:, cols].astype(f32) + total.astype(jnp.bfloat16).astype(f32)
    flt = flt.astype(jnp.bfloat16).astype(f32)
    resid[...] = flt.astype(jnp.bfloat16)
    gained = flt * gain[:, cols]
    ones = jnp.ones((8, flt.shape[1]), f32)
    high = lax.Precision.HIGHEST
    turned = (((1,), (1,)), ((), ()))
    square = lax.dot_general(ones, flt * flt, turned, precision=high, preferred_element_type=f32)
    logit = lax.dot_general(
        ones, gained * gate[:, cols].astype(f32), turned, precision=high, preferred_element_type=f32
    )
    rows = flt.shape[0]
    stats[0, 0, :, :rows] = square
    stats[0, 1, :, :rows] = logit
    copies = exchange(stats.at[0], stats, send2, recv2)
    for copy in copies:
        copy.wait()
    both = stats[0]
    for k in range(1, tp_count):
        both = both + stats[k]
    scale = lax.rsqrt(both[0, :, :rows] / width + 1e-06)
    branch[...] = route[...]
    branch[:1, :rows] = jax.nn.sigmoid(scale * both[1, :, :rows])[:1]
    first = (lax.broadcasted_iota(jnp.int32, (8, flt.shape[1]), 0) == 0).astype(f32)
    column = lax.dot_general(
        scale, first, (((0,), (0,)), ((), ())), precision=high, preferred_element_type=f32
    )
    value = (gained * column).astype(jnp.bfloat16)
    half = rows // 2
    normed[0] = value[:half]
    normed[1] = value[half:]


def mix(reads, weights, tokens, gain, gate, route, tp_count, width):
    rows, cols = tokens.shape[0], tokens.shape[1] // tp_count
    bf16, f32 = jnp.bfloat16, jnp.float32
    return pl.pallas_call(
        functools.partial(mix_kernel, tp_count, width),
        out_shape=(
            jax.ShapeDtypeStruct((2, rows // 2, cols), bf16),
            jax.ShapeDtypeStruct((rows, cols), bf16),
            jax.ShapeDtypeStruct((8, 128), f32),
        ),
        in_specs=vmem(6),
        out_specs=tuple(vmem(3)),
        scratch_shapes=[
            pltpu.VMEM((tp_count, *reads.shape), bf16),
            pltpu.VMEM((tp_count, 2, 8, 128), f32),
        ]
        + [pltpu.SemaphoreType.DMA((tp_count - 1,))] * 4,
        compiler_params=params(1),
        name="mix",
    )(reads, weights, tokens, gain, gate, route)


def greet_all(places, tp):
    barrier = pltpu.get_barrier_semaphore()
    for name in EP:
        for step in (1, -1):
            device = places.device((name, step))
            pl.semaphore_signal(barrier, inc=1, device_id=device, device_id_type=MESH)
    for move in (("y", 1), ("y", -1), ("core", 1)):
        pl.semaphore_signal(barrier, inc=1, device_id=tp.device(move), device_id_type=MESH)
    pl.semaphore_wait(barrier, 7)


def chosen(info, expert, seq, span, offset):
    lane = lax.broadcasted_iota(jnp.int32, (1, 128), 1)
    before = lax.broadcasted_iota(jnp.int32, (128, 128), 0) < lax.broadcasted_iota(
        jnp.int32, (128, 128), 1
    )
    slot_at = lax.broadcasted_iota(jnp.int32, (span, 128), 0).astype(jnp.float32)
    named = (info[1:2] == expert) | (info[2:3] == expert)
    named = jnp.where(named & (lane < seq), 1.0, 0.0)
    slot = jnp.dot(
        jnp.broadcast_to(named, (8, 128)),
        before.astype(jnp.float32),
        preferred_element_type=jnp.float32,
    )[:1]
    place = jnp.where(named > 0, slot + float(offset), -1.0)
    return jnp.where(place == slot_at, 1.0, 0.0)


def forward_plan(sizes, tp_count):
    big = timed(ep_tree(sizes), 1.06, LAG_EP)
    small = timed([n for n in ep_tree(sizes) if n.chunk == 0], 0.1, LAG_EP)
    ready = {}
    for node in big + small:
        dz = node.off[0] % sizes[0]
        ready[dz] = max(ready.get(dz, 0.0), node.came)
    ranks, base = [], 0.0
    for dz in sorted(ready, key=lambda d: ready[d]):
        base = max(ready[dz] + 1.0, base + GAP)
        ranks.append((dz, base))
    flows = []
    for rank, (dz, base) in enumerate(ranks):
        trees = [timed(tp_tree(tp_count, 2, (rank % 2,)), cost, LAG_TP) for cost in (1.06, 0.8, 0.4)]
        flows.append((dz, base, trees))
    return big, small, flows


def forward_kernel(
    big, small, flows, sizes, tp_sizes, capacity,
    block, extra, both, gate_hbm, up_hbm, down_hbm,
    partial, hid_all, extra_all,
    out, wide, rows, full, mine, slots, sums, gate_w, up_w, down_w, gate_val, hidden,
    send, recv, send2, recv2, send3, recv3, send4, recv4, send5, recv5, loaded,
):
    f32, bf16 = jnp.float32, jnp.bfloat16
    loads = [
        pltpu.make_async_copy(src, dst, loaded.at[i])
        for i, (src, dst) in enumerate(((gate_hbm, gate_w), (up_hbm, up_w), (down_hbm, down_w)))
    ]
    for load in loads:
        load.start()
    places, tp = Places("ep", sizes), Places("tp", tp_sizes)
    greet_all(places, tp)
    mine_at = places.flat(places.me)
    expert = mine_at.astype(f32)
    me = tp.flat(tp.me)
    zs, xs = sizes
    _, half_rows, part = block.shape
    seq = 2 * half_rows
    span = capacity * xs
    half = hidden.shape[1]
    hid = both.shape[1] // 2
    mine[...] = jnp.zeros_like(mine)
    events, started = [], []
    out[mine_at] = block[...]
    extra_all[mine_at] = extra[...]
    started.append(
        gather_events(
            big, places, lambda c: block.at[c], lambda c, b: out.at[b, c], send, recv, events
        )
    )
    started.append(
        gather_events(
            small, places, lambda c: extra, lambda c, b: extra_all.at[b], send2, recv2, events, 0.1
        )
    )
    def columns(b):
        return pl.ds(pl.multiple_of(b * part, part), part)

    def use_group(rank, dz):
        first = pl.multiple_of(places.along(0, -dz) * xs, xs)
        picked = jnp.zeros((span, part), f32)
        for x in range(xs):
            info = extra_all[first + x]
            select = chosen(info, expert, seq, span, capacity * x)[:, :seq].astype(bf16)
            value = out[first + x].reshape(seq, part)
            picked = picked + jnp.dot(select, value, preferred_element_type=f32)
        rows[rank] = picked.astype(bf16)
        full[pl.ds(rank * span, span), columns(me)] = picked.astype(bf16)
        value = out[pl.ds(first, xs)].reshape(xs * seq, part)
        product = jnp.dot(value, both[...], preferred_element_type=f32).astype(bf16)
        wide[rank] = product.reshape(2 * xs, half_rows, product.shape[1])

    nodes = len(flows[0][2][0])
    row_time = []
    for rank, (dz, base, (row_tree, sum_tree, hid_tree)) in enumerate(flows):
        events.append((base - 0.1, functools.partial(use_group, rank, dz)))
        sems = [
            sem.at[pl.ds(rank * nodes, nodes)] for sem in (send3, recv3, send4, recv4, send5, recv5)
        ]

        def put(chunk, at, value, rank=rank):
            gate, up = value[:, :hid], value[:, hid:]
            mine[rank, at, :hid] = (gate * jax.nn.sigmoid(gate) * up).astype(bf16)

        started.append(
            reduce_events(
                sum_tree, tp,
                lambda c, b, r=rank: wide.at[r, b],
                lambda c, b, at, r=rank: wide[r, b, at, :],
                put, slots.at[rank], sums.at[rank], half_rows, sems[2], sems[3], events, base,
            )
        )
        summed = base + max(node.came for node in sum_tree)
        started.append(
            gather_events(
                row_tree, tp,
                lambda c, r=rank: rows.at[r],
                lambda c, b, r=rank: full.at[pl.ds(r * span, span), columns(b)],
                sems[0], sems[1], events, base + 0.01,
            )
        )
        row_time.append(base + 0.01 + max(node.came for node in row_tree))

        def keep(rank, dz):
            hid_all[places.along(0, -dz), me] = mine[rank]

        events.append((summed + 0.01, functools.partial(keep, rank, dz)))

        def hid_target(c, b, dz=dz):
            return hid_all.at[places.along(0, -dz), b]

        started.append(
            gather_events(
                hid_tree, tp, lambda c, r=rank: mine.at[r], hid_target,
                sems[4], sems[5], events, summed + 0.02,
            )
        )

    group_rows = full.shape[0] // 2

    def gate_part(h):
        if h == 0:
            loads[0].wait()
        value = full[pl.ds(h * group_rows, group_rows), :]
        gate_val[...] = jnp.dot(value, gate_w[...], preferred_element_type=f32)

    def up_part(h):
        if h == 0:
            loads[1].wait()
        value = full[pl.ds(h * group_rows, group_rows), :]
        up_val = jnp.dot(value, up_w[...], preferred_element_type=f32)
        gate = gate_val[...]
        hidden[...] = (gate * jax.nn.sigmoid(gate) * up_val).astype(bf16)

    def down_part(h, piece, pieces):
        if h == 0 and piece == 0:
            loads[2].wait()
        width = partial.shape[2] // pieces
        at = slice(piece * width, (piece + 1) * width)
        product = jnp.dot(hidden[...], down_w[:, at], preferred_element_type=f32)
        partial[h, :, at] = product.astype(bf16)

    for h in range(2):
        when = max(row_time[h * len(flows) // 2 : (h + 1) * len(flows) // 2]) + 0.02
        if h == 1:
            when = max(when, max(at for at, _ in events) + 0.02)
        step = 1.5
        events.append((when, functools.partial(gate_part, h)))
        events.append((when + step, functools.partial(up_part, h)))
        for piece in range(4):
            act = functools.partial(down_part, h, piece, 4)
            events.append((when + step * 2 + piece * step / 2, act))
    run_events(events, started)


def forward(block, extra, both, gate_w, up_w, down_w, sizes, tp_count, capacity):
    count = sizes[0] * sizes[1]
    tp_sizes = (tp_count // 2, 2)
    big, small, flows = forward_plan(sizes, tp_count)
    bf16, f32 = block.dtype, jnp.float32
    _, half_rows, part = block.shape
    span = capacity * sizes[1]
    slots = capacity * count
    width = part * tp_count
    half = gate_w.shape[1]
    hid = both.shape[1] // 2
    lanes = -(-hid // 128) * 128
    groups = sizes[0]
    nodes = groups * len(flows[0][2][0])
    anywhere = [pl.BlockSpec(memory_space=pl.ANY)] * 3
    return pl.pallas_call(
        functools.partial(forward_kernel, big, small, flows, sizes, tp_sizes, capacity),
        out_shape=(
            jax.ShapeDtypeStruct((2, slots // 2, width), bf16),
            jax.ShapeDtypeStruct((groups, tp_count, half_rows, lanes), bf16),
            jax.ShapeDtypeStruct((count, *extra.shape), f32),
        ),
        in_specs=vmem(3) + anywhere,
        out_specs=tuple(vmem(3)),
        scratch_shapes=[
            pltpu.VMEM((count, 2, half_rows, part), bf16),
            pltpu.VMEM((groups, tp_count, half_rows, 2 * hid), bf16),
            pltpu.VMEM((groups, span, part), bf16),
            pltpu.VMEM((slots, width), bf16),
            pltpu.VMEM((groups, half_rows, lanes), bf16),
            pltpu.VMEM((groups, nodes // groups, half_rows, 2 * hid), bf16),
            pltpu.VMEM((groups, nodes // groups, half_rows, 2 * hid), bf16),
            pltpu.VMEM(gate_w.shape, bf16),
            pltpu.VMEM(up_w.shape, bf16),
            pltpu.VMEM(down_w.shape, bf16),
            pltpu.VMEM((slots // 2, half), f32),
            pltpu.VMEM((slots // 2, half), bf16),
        ]
        + dma_sems(big)
        + dma_sems(small)
        + [pltpu.SemaphoreType.DMA((nodes,))] * 6
        + [pltpu.SemaphoreType.DMA((3,))],
        compiler_params=params(2),
        name="forward",
    )(block, extra, both, gate_w, up_w, down_w)


def backward_plan(sizes, tp_count):
    big = timed(ep_tree(sizes), 1.06, LAG_EP)
    last = max(node.came for node in big)
    ready = {}
    for node in big:
        dz = node.off[0] % sizes[0]
        ready[dz] = max(ready.get(dz, 0.0), node.came)
    flows, base, start = [], 0.0, 0.0
    for rank, dz in enumerate(sorted(ready, key=lambda d: -ready[d])):
        tree = timed(tp_tree(tp_count, 2, (rank % 2,)), 1.06, LAG_BACK)
        done = base + max(node.came for node in tree) + 0.5
        start = max(start, done - (last - ready[dz]))
        flows.append((dz, base, done, tree))
        base += 1.8
    return big, flows, start + 0.1


def backward_kernel(
    big, flows, start, spots, sizes, tp_sizes, capacity,
    partial, extra_all, hid_all, down, resid, output,
    slots, sums, answer, dense, mine, slots2, sums2, send, recv, send2, recv2,
):
    f32, bf16 = jnp.float32, jnp.bfloat16
    places, tp = Places("ep", sizes), Places("tp", tp_sizes)
    greet_all(places, tp)
    expert = places.flat(places.me).astype(f32)
    zs, xs = sizes
    _, half_rows, part = resid.shape
    seq = 2 * half_rows
    span = capacity * xs
    events, started = [], []
    nodes = len(flows[0][3])
    per_half = partial.shape[1] // span

    def columns(b):
        return pl.ds(pl.multiple_of(b * part, part), part)

    own = (
        lax.broadcasted_iota(jnp.int32, (seq, 128), 0)
        == lax.broadcasted_iota(jnp.int32, (seq, 128), 1)
    ).astype(f32)

    def dense_group(rank, dz):
        group = places.along(0, -dz)
        first = group * xs
        value = hid_all[group].reshape(xs * seq, hid_all.shape[3])
        product = jnp.dot(value, down[...], preferred_element_type=f32)
        for x in range(xs):
            branch = jnp.sum(own * extra_all[first + x][:1], axis=1, keepdims=True)
            dense[rank, x] = product[x * seq : (x + 1) * seq] * branch

    def combine(rank, dz):
        first = places.along(0, -dz) * xs
        picks, weight = [], jnp.zeros((span, 1), f32)
        for x in range(xs):
            info = extra_all[first + x]
            select = chosen(info, expert, seq, span, capacity * x)
            named = jnp.where(info[1:2] == expert, info[3:4], 0.0)
            named = named + jnp.where(info[2:3] == expert, info[4:5], 0.0)
            weight = weight + jnp.sum(select * named, axis=1, keepdims=True)
            picks.append(select[:, :seq].astype(bf16))
        value = (answer[rank] * weight).astype(bf16)
        for x in range(xs):
            routed = lax.dot_general(
                picks[x], value, (((0,), (0,)), ((), ())), preferred_element_type=f32
            )
            total = (routed + dense[rank, x]).astype(bf16)
            mine[first + x] = total.reshape(2, half_rows, part)

    for rank, (dz, base, done, tree) in enumerate(flows):
        spot = spots[dz]
        half, at_row = spot // per_half, (spot % per_half) * span

        def put(chunk, at, value, rank=rank):
            answer[rank, at, :] = value.astype(bf16).astype(f32)

        started.append(
            reduce_events(
                tree, tp,
                lambda c, b, h=half, r=at_row: partial.at[h, pl.ds(r, span), columns(b)],
                lambda c, b, at, h=half, r=at_row: partial[
                    h, pl.ds(r + at.start, at.size), columns(b)
                ],
                put, slots.at[rank], sums.at[rank], span,
                send.at[pl.ds(rank * nodes, nodes)], recv.at[pl.ds(rank * nodes, nodes)],
                events, base,
            )
        )
        events.append((base + 1.0, functools.partial(dense_group, rank, dz)))
        events.append((done, functools.partial(combine, rank, dz)))

    def finish(c, at, value):
        output[c, at, :] = (resid[c, at, :].astype(f32) + value).astype(output.dtype)

    started.append(
        reduce_events(
            big, places, lambda c, b: mine.at[b, c], lambda c, b, at: mine[b, c, at, :], finish,
            slots2, sums2, half_rows, send2, recv2, events, start,
        )
    )
    run_events(events, started)


def backward(partial, extra_all, hid_all, down, resid, sizes, tp_count, capacity):
    big, flows, start = backward_plan(sizes, tp_count)
    order = [dz for dz, _, _ in forward_plan(sizes, tp_count)[2]]
    spots = {dz: at for at, dz in enumerate(order)}
    bf16, f32 = partial.dtype, jnp.float32
    _, half_rows, part = resid.shape
    span = capacity * sizes[1]
    groups, nodes = sizes[0], len(flows[0][3])
    count = sizes[0] * sizes[1]
    return pl.pallas_call(
        functools.partial(
            backward_kernel, big, flows, start, spots, sizes, (tp_count // 2, 2), capacity
        ),
        out_shape=jax.ShapeDtypeStruct(resid.shape, bf16),
        in_specs=vmem(5),
        out_specs=vmem(1)[0],
        scratch_shapes=[
            pltpu.VMEM((groups, nodes, span, part), bf16),
            pltpu.VMEM((groups, nodes, span, part), bf16),
            pltpu.VMEM((groups, span, part), f32),
            pltpu.VMEM((groups, sizes[1], 2 * half_rows, part), f32),
            pltpu.VMEM((count, 2, half_rows, part), bf16),
            pltpu.VMEM((len(big), half_rows, part), bf16),
            pltpu.VMEM((len(big), half_rows, part), bf16),
        ]
        + [pltpu.SemaphoreType.DMA((groups * nodes,))] * 2
        + dma_sems(big),
        compiler_params=params(4),
        name="backward",
    )(partial, extra_all, hid_all, down, resid)


def split_up(x, dim, peers):
    before, after = (x.shape[:dim], x.shape[dim + 1 :])
    return jnp.moveaxis(x.reshape(*before, peers, -1, *after), dim, 0)


def rms_norm(values, gain):
    flt = values.astype(jnp.float32)
    scaled = flt * lax.rsqrt(jnp.mean(flt * flt, axis=-1, keepdims=True) + 1e-06)
    return (scaled * gain).astype(jnp.bfloat16)


def discretize(decay_rate, frequency, log_step, b_real, b_imag):
    step_size = jnp.exp(log_step)[:, None]
    lam_re = -decay_rate
    magnitude = jnp.exp(lam_re * step_size)
    abar_re = magnitude * jnp.cos(frequency * step_size)
    abar_im = magnitude * jnp.sin(frequency * step_size)
    denom = lam_re * lam_re + frequency * frequency
    fac_re = ((abar_re - 1.0) * lam_re + abar_im * frequency) / denom
    fac_im = (abar_im * lam_re - (abar_re - 1.0) * frequency) / denom
    bbar_re = fac_re[..., None] * b_real - fac_im[..., None] * b_imag
    bbar_im = fac_re[..., None] * b_imag + fac_im[..., None] * b_real
    return (abar_re, abar_im, bbar_re, bbar_im)


def state_step(
    drive, states, decay_rate, frequency, log_step, b_real, b_imag, c_real, c_imag, skip_gain
):
    count = drive.shape[0]
    groups = decay_rate.shape[0]
    abar_re, abar_im, bbar_re, bbar_im = discretize(decay_rate, frequency, log_step, b_real, b_imag)
    grouped = drive.astype(jnp.float32).reshape(count, groups, GROUP)
    old_re = states[0].reshape(count, groups, STATE)
    old_im = states[1].reshape(count, groups, STATE)
    push_re = jnp.einsum("ngh,gph->ngp", grouped, bbar_re)
    push_im = jnp.einsum("ngh,gph->ngp", grouped, bbar_im)
    new_re = abar_re * old_re - abar_im * old_im + push_re
    new_im = abar_re * old_im + abar_im * old_re + push_im
    readout = (
        jnp.einsum("ngp,ghp->ngh", new_re, c_real)
        - jnp.einsum("ngp,ghp->ngh", new_im, c_imag)
        + skip_gain.reshape(groups, GROUP) * grouped
    )
    reads = jax.nn.gelu(readout.reshape(count, groups * GROUP)).astype(jnp.bfloat16)
    fresh = jnp.stack(
        [new_re.reshape(count, groups * STATE), new_im.reshape(count, groups * STATE)]
    )
    return (reads, fresh)


def shards(
    tokens,
    mix_gain,
    ffn_gain,
    in_proj,
    decay_rate,
    frequency,
    log_step,
    b_real,
    b_imag,
    c_real,
    c_imag,
    skip_gain,
    states,
    out_proj,
    route_ids,
    route_logits,
    expert_gate,
    expert_up,
    expert_down,
    dense_gate,
    dense_up,
    dense_down,
    branch_gate,
):
    seq_count, width = tokens.shape
    tp_count = lax.axis_size("tp")
    ep_count = lax.axis_size(EP)
    tp_index = lax.axis_index("tp")
    ep_index = lax.axis_index(EP)
    part_width = width // tp_count
    f32, bf16 = jnp.float32, jnp.bfloat16
    top_count = route_ids.shape[1]
    capacity = max(2, 2 * seq_count * top_count // ep_count)
    slots = ep_count * capacity

    route_weights = jax.nn.softmax(route_logits, axis=-1)
    route_rows = jnp.zeros((8, 128), f32)
    route_rows = route_rows.at[1 : 1 + top_count, :seq_count].set(route_ids.astype(f32).T)
    weight_at = 1 + top_count
    route_rows = route_rows.at[weight_at : weight_at + top_count, :seq_count].set(route_weights.T)

    out_cols = lax.all_to_all(split_up(out_proj, 1, tp_count), "tp", 0, 0, tiled=True)
    out_cols = out_cols.reshape(tp_count * out_proj.shape[0], part_width)

    normed = rms_norm(tokens, mix_gain)
    drive = jnp.dot(normed, in_proj, preferred_element_type=f32).astype(bf16)
    reads, new_states = state_step(
        drive, states, decay_rate, frequency, log_step, b_real, b_imag, c_real, c_imag, skip_gain
    )
    normed_two, resid, branch = mix(
        reads, out_cols, tokens, ffn_gain[None], branch_gate[None], route_rows, tp_count, width
    )
    sizes = (lax.axis_size("ep_0"), lax.axis_size("ep_1"))
    both_proj = jnp.concatenate([dense_gate, dense_up], axis=1)
    partial, dense_hidden, branch_all = forward(
        normed_two, branch, both_proj, expert_gate[0], expert_up[0], expert_down[0],
        sizes, tp_count, capacity,
    )
    spare = dense_hidden.shape[3] - dense_down.shape[0]
    dense_down = jnp.pad(dense_down, ((0, spare), (0, 0)))
    output = backward(
        partial, branch_all, dense_hidden, dense_down,
        resid.reshape(2, seq_count // 2, part_width), sizes, tp_count, capacity,
    )
    return (output.reshape(seq_count, part_width), new_states)


def solution(mesh):
    finer = Mesh(mesh.devices.reshape(8, 4, mesh.shape["tp"]), ("ep_0", "ep_1", "tp"))
    return jax.shard_map(
        shards,
        mesh=finer,
        in_specs=(
            P(EP, None),
            P(),
            P(),
            P(None, "tp"),
            P("tp", None),
            P("tp", None),
            P("tp"),
            P("tp", None, None),
            P("tp", None, None),
            P("tp", None, None),
            P("tp", None, None),
            P("tp"),
            P(None, EP, "tp"),
            P("tp", None),
            P(EP, None),
            P(EP, None),
            P(EP, None, "tp"),
            P(EP, None, "tp"),
            P(EP, "tp", None),
            P("tp", EP),
            P("tp", EP),
            P(EP, "tp"),
            P(),
        ),
        out_specs=(P(EP, "tp"), P(None, EP, "tp")),
        check_vma=False,
    )
```
